256 devices in a mesh: grp: 2 (over y), tp: 16 (over z), dp: 8 (over x, core).
Axes of the slice: x: 4, y: 2, z: 16, core: 2. Of those that a mesh axis runs over, the one named last changes fastest.
The devices are a block of a 4x16x16 slice.
Arguments:
- skip_path_activations: bfloat16 [256, 8, 4096], P('grp', None, 'dp'), parts along dimension 0
- novel_lengths_per_sequence: int32 [256], P(('grp', 'dp')), parts along dimension 0, may hold values from 1 to 8, 512 in all
- input_normalizer_scales: bfloat16 [2, 4096], P(None, 'dp'), may hold values from 0.099609375 to 1.8984375
- question_projector: bfloat16 [2, 4096, 2048], P(None, 'dp', 'tp'), may hold values from -0.09375 to 0.09375
- lookup_projector: bfloat16 [2, 4096, 2048], P(None, 'dp', 'tp'), may hold values from -0.09375 to 0.09375
- payload_projector: bfloat16 [2, 4096, 4096], P(None, 'dp', 'tp'), may hold values from -0.09375 to 0.09375
- emitted_valve_projector: bfloat16 [2, 4096, 4096], P(None, 'dp', 'tp'), may hold values from -0.09375 to 0.09375
- keeping_valve_projector: bfloat16 [2, 4096, 2048], P(None, 'dp', 'tp'), may hold values from -0.09375 to 0.09375
- keeping_valve_shift: float32 [2, 2048], P(None, 'tp'), may hold values from -3 to 6
- additional_dwindle_exponent: float32 [256, 8, 16], P(('grp', 'dp'), None, 'tp'), parts along dimension 0, may hold values from -0.7 to 0
- headwise_normalizer_scales: bfloat16 [2, 256], replicated, may hold values from 0.099609375 to 1.8984375
- closing_projector: bfloat16 [2, 4096, 4096], P(None, 'tp', 'dp'), may hold values from -0.1875 to 0.1875
- earlier_recurrence_grid: float32 [2, 256, 16, 128, 256], P(None, ('grp', 'dp'), 'tp'), parts along dimension 1, may hold values from -6 to 6
Outputs:
- stream_out: bfloat16 [256, 8, 4096], P('grp', None, 'dp'), parts along dimension 0
- state_out: float32 [2, 256, 16, 128, 256], P(None, ('grp', 'dp'), 'tp'), parts along dimension 1
The draws below stay inside these ranges and needn't reach their ends.
There are 2 independent parts, one for each index of `grp`. The reference program is written for one: setup_inputs(seed, part) draws one part's arguments, and reference() takes and returns one part's arrays. A program takes and returns all parts, laid end to end along the dimension named above; an argument that names none is the same for every part. Nothing has to cross between parts.
Inputs may be any that keep to these rules, and one draw needn't show every extreme that they name: `novel_lengths_per_sequence`: each sequence has 1 to 8 live token slots, the first ones; some sequence has 8. In each group the live slots of its 128 sequences add up to half of 128 times 8.
All inputs are finite; a program needn't handle non-finite values.
Results may differ from the reference program's by a relative error of at most 0.024.
Values may be sent and summed in bfloat16 or wider, within the bound.
No kernel may reach another device: no remote copies, remote signals or barrier semaphores. Data moves between devices by JAX's collectives and lax.ppermute only.
A program may use at most 64 MiB of HBM per device.

```python
import math
import jax
import jax.numpy as jnp
import numpy as np
from jax import lax

MODEL_BREADTH = 4096
HEADS = 16
DK = 128
DV = 256
LAYERS = 2
NEW = 8
QK = 2048
VW = 4096
BATCH = 128
N_DP = 8


def draw_skip_path_activations(key, part):
    first = jax.random.fold_in(jax.random.fold_in(key, 11), 0)
    column_scale = 0.5 * 10.0 ** (jnp.arange(MODEL_BREADTH, dtype=jnp.float32) / MODEL_BREADTH)
    values = jnp.clip(jax.random.normal(first, (BATCH, NEW, MODEL_BREADTH), jnp.float32), -6.0, 6.0) * column_scale
    return values.astype(jnp.bfloat16)


def draw_keeping_valve_shift(key, part):
    first, second, third = jax.random.split(jax.random.fold_in(key, 23), 3)
    share = 0.5
    quick = jax.random.uniform(first, (LAYERS, QK), jnp.float32) < share
    quick_value = jax.random.uniform(second, (LAYERS, QK), jnp.float32, -3.0, 0.0)
    slow_value = jax.random.uniform(third, (LAYERS, QK), jnp.float32, 2.0, 6.0)
    return jnp.where(quick, quick_value, slow_value)


def draw_additional_dwindle_exponent(key, part):
    first, second = jax.random.split(jax.random.fold_in(key, 37))
    hit = jax.random.randint(first, (BATCH, NEW, HEADS), 0, 12) == 0
    amount = jnp.log(jax.random.uniform(second, (BATCH, NEW, HEADS), jnp.float32, 0.5, 0.8))
    return jnp.where(hit, amount, 0.0).astype(jnp.float32)


def levels(stream_key, extent, cuts, smallest, high):
    def one(axis_at, blocks):
        draws = jax.random.uniform(jax.random.fold_in(jax.random.fold_in(stream_key, 6), axis_at), (blocks,), jnp.float32, smallest / len(cuts), high / len(cuts))
        return jnp.repeat(jnp.exp(draws), extent[axis_at] // blocks).reshape((-1,) + (1,) * (len(extent) - axis_at - 1))

    factor_of = one(*cuts[0])
    for cut in cuts[1:]:
        factor_of = factor_of * one(*cut)
    return factor_of


def split_up(number_of, total, bound, lean):
    weights = [(1 << 20) // math.isqrt(grade ** lean) + 1 for grade in range(2, number_of + 1)]
    rest, given = total - bound - (number_of - 1), [1] * (number_of - 1)
    while rest > 0:
        movable = [i for i in range(number_of - 1) if given[i] < bound]
        mass, left = sum([weights[i] for i in movable]), rest
        for i in movable:
            addition = min(bound - given[i], max(1, left * weights[i] // mass), rest)
            given[i] = given[i] + addition
            rest = rest - addition
    return np.array([bound] + given)


def ragged(rng, number_of, total, reach, slope):
    if number_of == 2:
        one = jax.random.randint(rng, (), max(1, total - reach), min(reach, total - 1) + 1)
        return jnp.stack([one, total - one])
    lengths = jnp.asarray(split_up(number_of, total, reach, slope), jnp.int32)
    couples = (number_of - 1) // 2
    source_of, receiver = lengths[1:1 + 2 * couples:2], lengths[2:2 + 2 * couples:2]
    slack = jnp.minimum(source_of - 1, reach - receiver)
    passed = jax.random.randint(jax.random.fold_in(rng, 1), (couples,), 0, 1 << 20) % (slack + 1)
    lengths = lengths.at[1:1 + 2 * couples:2].set(source_of - passed).at[2:2 + 2 * couples:2].set(receiver + passed)
    return lengths[jax.random.permutation(jax.random.fold_in(rng, 2), number_of)]


def noise(stream_key, shape, scale, bound, shards=(), kind=jnp.bfloat16):
    array = scale * jax.random.normal(stream_key, shape, jnp.float32)
    if shards:
        array = array * levels(stream_key, shape, shards, -0.22, 0.18)
    return jnp.clip(array, -bound, bound).astype(kind)


def setup_inputs(seed: int = 0, part: int = 0) -> dict:
    arg_keys = jax.random.split(jax.random.key(seed), 14)
    part_keys = jax.random.split(jax.random.fold_in(arg_keys[13], part), 14)
    skip_path_activations = draw_skip_path_activations(jax.random.fold_in(jax.random.fold_in(arg_keys[13], part), 71), part)
    novel_lengths_per_sequence = ragged(part_keys[1], BATCH, BATCH * NEW // 2, NEW, 2).astype(jnp.int32)
    input_normalizer_scales = jnp.clip(1.0 + 0.18 * jax.random.normal(arg_keys[2], (LAYERS, MODEL_BREADTH), jnp.float32), 0.099609375, 1.8984375).astype(jnp.bfloat16)
    question_projector = noise(arg_keys[3], (LAYERS, MODEL_BREADTH, QK), MODEL_BREADTH ** -0.5, 0.09375, ((1, 8), (2, 16)))
    lookup_projector = noise(arg_keys[4], (LAYERS, MODEL_BREADTH, QK), MODEL_BREADTH ** -0.5, 0.09375, ((1, 8), (2, 16)))
    payload_projector = noise(arg_keys[5], (LAYERS, MODEL_BREADTH, VW), MODEL_BREADTH ** -0.5, 0.09375, ((1, 8), (2, 16)))
    emitted_valve_projector = noise(arg_keys[6], (LAYERS, MODEL_BREADTH, VW), MODEL_BREADTH ** -0.5, 0.09375, ((1, 8), (2, 16)))
    keeping_valve_projector = noise(arg_keys[7], (LAYERS, MODEL_BREADTH, QK), MODEL_BREADTH ** -0.5, 0.09375, ((1, 8), (2, 16)))
    keeping_valve_shift = draw_keeping_valve_shift(jax.random.fold_in(arg_keys[13], 71), part)
    additional_dwindle_exponent = draw_additional_dwindle_exponent(jax.random.fold_in(jax.random.fold_in(arg_keys[13], part), 71), part)
    headwise_normalizer_scales = jnp.clip(1.0 + 0.18 * jax.random.normal(arg_keys[10], (LAYERS, DV), jnp.float32), 0.099609375, 1.8984375).astype(jnp.bfloat16)
    closing_projector = noise(arg_keys[11], (LAYERS, VW, MODEL_BREADTH), (VW // 4) ** -0.5, 0.1875, ((1, 16), (2, 8)))
    earlier_recurrence_grid = noise(part_keys[12], (LAYERS, BATCH, HEADS, DK, DV), 1.0, 6.0, ((1, 8), (2, 16)), jnp.float32)
    return {"skip_path_activations": skip_path_activations, "novel_lengths_per_sequence": novel_lengths_per_sequence, "input_normalizer_scales": input_normalizer_scales, "question_projector": question_projector, "lookup_projector": lookup_projector, "payload_projector": payload_projector, "emitted_valve_projector": emitted_valve_projector, "keeping_valve_projector": keeping_valve_projector, "keeping_valve_shift": keeping_valve_shift, "additional_dwindle_exponent": additional_dwindle_exponent, "headwise_normalizer_scales": headwise_normalizer_scales, "closing_projector": closing_projector, "earlier_recurrence_grid": earlier_recurrence_grid}


EPS = 1e-06
TAU = 16.0

def scaled_rms(values_f, gain):
    return values_f * lax.rsqrt(lax.optimization_barrier(jnp.mean(values_f * values_f, axis=-1, keepdims=True)) + EPS) * gain.astype(jnp.float32)

def round_trip(values_f):
    return lax.optimization_barrier(values_f.astype(jnp.bfloat16)).astype(jnp.float32)

def split_dot(normed, weight):
    number_of_lines = normed.shape[0]
    blocks = normed.astype(jnp.float32).reshape(number_of_lines, N_DP, MODEL_BREADTH // N_DP)
    pieces = weight.astype(jnp.float32).reshape(N_DP, MODEL_BREADTH // N_DP, weight.shape[1])
    partial_value = jnp.einsum('rnk,nkc->nrc', blocks, pieces, precision=lax.Precision.HIGHEST)
    return round_trip(partial_value).sum(axis=0)

def advance(query_rows, key_rows, value_rows, fade_log_amount, carried):
    steps_n = query_rows.shape[1]
    cumulative = jnp.cumsum(fade_log_amount, axis=1)
    spread = cumulative[:, :, None] - cumulative[:, None, :]
    causal = jnp.tril(jnp.ones((steps_n, steps_n), dtype=bool))
    decay_mat = jnp.exp(jnp.where(causal[None, :, :, None, None], spread, -jnp.inf))
    scores = jnp.einsum('sihd,sjhd,sijhd->shij', query_rows, key_rows, decay_mat, precision=lax.Precision.HIGHEST)
    within = jnp.einsum('shij,sjhv->sihv', scores, value_rows, precision=lax.Precision.HIGHEST)
    carried_part = jnp.einsum('sihd,shdv->sihv', query_rows * jnp.exp(cumulative), carried, precision=lax.Precision.HIGHEST)
    final_log = cumulative[:, -1]
    weighted = key_rows * jnp.exp(final_log[:, None] - cumulative)
    updated = jnp.exp(final_log)[..., None] * carried + jnp.einsum('sjhd,sjhv->shdv', weighted, value_rows, precision=lax.Precision.HIGHEST)
    return (within + carried_part, updated)

def reference(skip_path_activations, novel_lengths_per_sequence, input_normalizer_scales, question_projector, lookup_projector, payload_projector, emitted_valve_projector, keeping_valve_projector, keeping_valve_shift, additional_dwindle_exponent, headwise_normalizer_scales, closing_projector, earlier_recurrence_grid):
    number_of_lines = BATCH * NEW
    ongoing = skip_path_activations.reshape(number_of_lines, MODEL_BREADTH)
    live_entry_indicator = (jnp.arange(NEW, dtype=jnp.int32)[None, :] < novel_lengths_per_sequence[:, None]).astype(jnp.float32)
    new_states = []
    for block_index in range(LAYERS):
        normed = scaled_rms(ongoing.astype(jnp.float32), input_normalizer_scales[block_index]).astype(jnp.bfloat16)
        query_rows = round_trip(split_dot(normed, question_projector[block_index])) * DK ** (-0.5)
        key_rows = round_trip(split_dot(normed, lookup_projector[block_index]))
        value_rows = round_trip(split_dot(normed, payload_projector[block_index]))
        gate_rows = round_trip(split_dot(normed, emitted_valve_projector[block_index]))
        logits = split_dot(normed, keeping_valve_projector[block_index])
        fade_log_amount = (jax.nn.log_sigmoid(logits + keeping_valve_shift[block_index]) / TAU).reshape(BATCH, NEW, HEADS, DK)
        fade_log_amount = (fade_log_amount + additional_dwindle_exponent[..., None]) * live_entry_indicator[:, :, None, None]
        key_rows = key_rows.reshape(BATCH, NEW, HEADS, DK) * live_entry_indicator[:, :, None, None]
        output, updated = advance(query_rows.reshape(BATCH, NEW, HEADS, DK), key_rows, value_rows.reshape(BATCH, NEW, HEADS, DV), fade_log_amount, earlier_recurrence_grid[block_index])
        new_states.append(updated)
        normed_out = scaled_rms(output, headwise_normalizer_scales[block_index]).reshape(number_of_lines, VW)
        gated_rows = (normed_out * jax.nn.silu(gate_rows) * live_entry_indicator.reshape(number_of_lines, 1)).astype(jnp.bfloat16)
        mixed = jnp.dot(gated_rows, closing_projector[block_index], preferred_element_type=jnp.float32)
        ongoing = (ongoing.astype(jnp.float32) + mixed).astype(jnp.bfloat16)
    return (ongoing.reshape(BATCH, NEW, MODEL_BREADTH), jnp.stack(new_states, axis=0))
```

```python
import functools

import jax
import jax.numpy as jnp
from jax import lax
from jax.experimental import pallas as pl
from jax.experimental.pallas import tpu as pltpu
from jax.sharding import PartitionSpec as P

LAYERS = 2
EPS = 1e-06
TAU = 16.0
BF = jnp.bfloat16
F32 = jnp.float32
VMEM_LIMIT = 56 * 1024 * 1024
ROUNDS = 4
SIDE = 128


def dot(a, b):
    return jnp.dot(a, b, preferred_element_type=F32)


def params(*semantics):
    return pltpu.CompilerParams(vmem_limit_bytes=VMEM_LIMIT, dimension_semantics=semantics or None)


def whole(shape):
    return pl.BlockSpec(shape, lambda *_: (0,) * len(shape))


def project(x, gain_ref, w_refs, a_ref, b_ref, lens_col):
    xf = x.astype(F32)
    scaled = jnp.clip(xf * gain_ref[...].astype(F32), -1e30, 1e30).astype(BF)
    wq, wk, wv, wr, wf = w_refs
    at = 0
    for w in (wq, wk, wv):
        a_ref[0, :, at : at + w.shape[-1]] = dot(scaled, w[0]).astype(BF)
        at += w.shape[-1]
    at = 0
    for w in (wr, wf):
        b_ref[0, :, at : at + w.shape[-1]] = dot(scaled, w[0]).astype(BF)
        at += w.shape[-1]
    squares = jnp.sum(xf * xf, axis=1, keepdims=True)
    high = squares.astype(BF).astype(F32)
    low = jnp.where(jnp.abs(high) < 3.0e38, squares - high, 0.0)
    lane = lax.broadcasted_iota(jnp.int32, (x.shape[0], SIDE), 1)
    side = jnp.where(lane == 0, high, jnp.where(lane == 1, low, 0.0))
    if lens_col is not None:
        side = jnp.where(lane == 2, lens_col, side)
    b_ref[0, :, at : at + SIDE] = side.astype(BF)


def project_first(local_seqs, meta, lens, x_ref, gain_ref, wq, wk, wv, wr, wf, a_ref, b_ref):
    rows = x_ref.shape[0]
    row = lax.broadcasted_iota(jnp.int32, (rows, SIDE), 0) - meta[9] * local_seqs
    lens_col = jnp.zeros((rows, SIDE), F32)
    for s in range(local_seqs):
        lens_col = jnp.where(row == s, lens[s].astype(F32), lens_col)
    project(x_ref[...], gain_ref, (wq, wk, wv, wr, wf), a_ref, b_ref, lens_col)


def piece_ids(meta, rows, tp, offset, sign):
    span = rows // ROUNDS
    lane = lax.broadcasted_iota(jnp.int32, (rows, rows), 1)
    block = lax.rem(meta[8] + offset + sign * ROUNDS * (lane // span) + 2 * tp, tp)
    return (block * span + lax.rem(lane, span)).astype(F32)


def expand(meta, tp, where_row, pieces):
    own, plus, minus, far_a, far_b = pieces
    rows = own.shape[0]
    half = far_a.shape[1]
    place = jnp.transpose(jnp.broadcast_to(where_row, (rows, where_row.shape[1])))
    at = jnp.broadcast_to(place[:, :1], (place.shape[0], rows))

    def pick(offset, piece):
        chosen = (at == piece_ids(meta, rows, tp, offset, -1)).astype(F32).astype(BF)
        return dot(chosen, piece)

    near = pick(0, own[...]) + pick(1, plus[...]) + pick(-1, minus[...])
    left = near[:, :half] + pick(2, far_a[...])
    right = near[:, half:] + pick(-2, far_b[...])
    return left, right, place


def project_next(tp, first, meta, where_ref, own, plus, minus, far_a, far_b, gain_ref, wq, wk, wv, wr, wf, a_ref, b_ref):
    owner = meta[first + pl.program_id(0)]
    left, right, _ = expand(meta, tp, where_ref[pl.ds(owner, 1), :], (own, plus, minus, far_a, far_b))
    x = jnp.concatenate([left, right], axis=1)
    project(x, gain_ref, (wq, wk, wv, wr, wf), a_ref, b_ref, None)


def finish(tp, meta, where_ref, own, plus, minus, far_a, far_b, x_ref, out_ref):
    left, right, place = expand(meta, tp, where_ref[pl.ds(pl.program_id(0), 1), :], (own, plus, minus, far_a, far_b))
    half = left.shape[1]
    dead = place[:, :1] < 0
    x = x_ref[...].astype(F32)
    out_ref[:, :half] = jnp.where(dead, x[:, :half], left).astype(BF)
    out_ref[:, half:] = jnp.where(dead, x[:, half:], right).astype(BF)


def weight_spec(layer, w):
    return pl.BlockSpec((1, w.shape[1], w.shape[2]), lambda i, *_: (layer, 0, 0))


def call_project_first(layer, first, meta, lens, x, gain, weights, blocks):
    rows, width = x.shape[0] // (2 * blocks), x.shape[1]
    a_cols = sum(w.shape[2] for w in weights[:3])
    b_cols = sum(w.shape[2] for w in weights[3:]) + SIDE
    return pl.pallas_call(
        functools.partial(project_first, lens.shape[0]),
        grid_spec=pltpu.PrefetchScalarGridSpec(
            num_scalar_prefetch=2,
            grid=(blocks,),
            in_specs=[
                pl.BlockSpec((rows, width), lambda i, meta, lens: (meta[first + i], 0)),
                whole((1, width)),
                *(weight_spec(layer, w) for w in weights),
            ],
            out_specs=[
                pl.BlockSpec((1, rows, a_cols), lambda i, *_: (i, 0, 0)),
                pl.BlockSpec((1, rows, b_cols), lambda i, *_: (i, 0, 0)),
            ],
        ),
        out_shape=[
            jax.ShapeDtypeStruct((blocks, rows, a_cols), BF),
            jax.ShapeDtypeStruct((blocks, rows, b_cols), BF),
        ],
        compiler_params=params("arbitrary"),
        name="project_first",
    )(meta, lens, x, gain[layer : layer + 1], *weights)


def piece_specs(pieces):
    return [whole(p.shape) for p in pieces]


def call_project_next(layer, first, tp, meta, where, pieces, gain, weights, blocks):
    rows, width = where.shape[1], gain.shape[1]
    a_cols = sum(w.shape[2] for w in weights[:3])
    b_cols = sum(w.shape[2] for w in weights[3:]) + SIDE
    return pl.pallas_call(
        functools.partial(project_next, tp, first),
        grid_spec=pltpu.PrefetchScalarGridSpec(
            num_scalar_prefetch=1,
            grid=(blocks,),
            in_specs=[
                whole(where.shape),
                *piece_specs(pieces),
                whole((1, width)),
                *(weight_spec(layer, w) for w in weights),
            ],
            out_specs=[
                pl.BlockSpec((1, rows, a_cols), lambda i, *_: (i, 0, 0)),
                pl.BlockSpec((1, rows, b_cols), lambda i, *_: (i, 0, 0)),
            ],
        ),
        out_shape=[
            jax.ShapeDtypeStruct((blocks, rows, a_cols), BF),
            jax.ShapeDtypeStruct((blocks, rows, b_cols), BF),
        ],
        compiler_params=params("arbitrary"),
        name="project_next",
    )(meta, where, *pieces, gain[layer : layer + 1], *weights)


def call_finish(tp, meta, where, pieces, x):
    owners, rows = where.shape
    return pl.pallas_call(
        functools.partial(finish, tp),
        grid_spec=pltpu.PrefetchScalarGridSpec(
            num_scalar_prefetch=1,
            grid=(owners,),
            in_specs=[
                whole(where.shape),
                *piece_specs(pieces),
                pl.BlockSpec((rows, x.shape[1]), lambda i, *_: (i, 0)),
            ],
            out_specs=pl.BlockSpec((rows, x.shape[1]), lambda i, *_: (i, 0)),
        ),
        out_shape=jax.ShapeDtypeStruct(x.shape, BF),
        compiler_params=params("arbitrary"),
        name="finish",
    )(meta, where, *pieces, x)


def recur(layer, full_width, with_plan, steps, lens, *refs):
    (ma, mb, ca, cb, ra, rb, ra2, rb2, shift_ref, extra_ref, hs_ref, state_hbm), rest = refs[:12], refs[12:]
    if with_plan:
        g_ref, wk_ref, v_ref, end_ref, where_ref, state, sem = rest
    else:
        g_ref, wk_ref, v_ref, end_ref, state, sem = rest
    load = pltpu.make_async_copy(state_hbm.at[layer], state, sem)
    load.start()
    seqs, key_dim, value_dim = state.shape
    rows = seqs * steps
    sum_a = (ma[0].astype(F32) + ca[0].astype(F32)) + (ra[0].astype(F32) + ra2[...].astype(F32))
    sum_b = (mb[0].astype(F32) + cb[0].astype(F32)) + (rb[0].astype(F32) + rb2[...].astype(F32))
    at = value_dim + key_dim
    side = sum_b[:, at : at + SIDE]
    squares = side[:, 0:1] + side[:, 1:2]
    rms = lax.rsqrt(squares / full_width + EPS)
    q = sum_a[:, :key_dim] * (rms * key_dim ** (-0.5))
    k = sum_a[:, key_dim : 2 * key_dim] * rms
    v = sum_a[:, 2 * key_dim :] * rms
    r = sum_b[:, :value_dim] * rms
    f = sum_b[:, value_dim:at] * rms

    row = lax.broadcasted_iota(jnp.int32, (rows, key_dim), 0)
    own_len = jnp.zeros((rows, key_dim), jnp.int32)
    for s in range(seqs):
        own_len = jnp.where(row // steps == s, lens[s], own_len)
    live = jnp.where(lax.rem(row, steps) < own_len, 1.0, 0.0)
    logits = f + shift_ref[...]
    log_sig = jnp.minimum(logits, 0.0) - jnp.log(1.0 + jnp.exp(-jnp.abs(logits)))
    fade = (log_sig / TAU + extra_ref[...]) * live
    k = k * live

    def by_seq(x):
        return x.reshape(seqs, steps, x.shape[1])

    q3, k3, v3, fade3 = by_seq(q), by_seq(k), by_seq(v), by_seq(fade)
    slot = lax.broadcasted_iota(jnp.int32, (seqs, steps, key_dim), 1)
    total = jnp.zeros_like(fade3)
    for j in range(steps):
        total = total + jnp.where(slot >= j, fade3[:, j : j + 1, :], 0.0)
    out = jnp.zeros_like(v3)
    for j in range(steps):
        apart = jnp.where(slot >= j, total - total[:, j : j + 1, :], -1e30)
        score = jnp.sum(q3 * k3[:, j : j + 1, :] * jnp.exp(apart), axis=-1, keepdims=True)
        out = out + score * v3[:, j : j + 1, :]
    last = total[:, steps - 1 : steps, :]
    wk_ref[...] = (k3 * jnp.exp(last - total)).reshape(rows, key_dim).astype(BF)
    v_ref[...] = v.astype(BF)
    end_ref[...] = jnp.exp(last)
    if with_plan:
        owners = where_ref.shape[0]
        n = side.shape[0]
        lens_all = jnp.where(lax.broadcasted_iota(jnp.int32, side.shape, 1) == 0, side[:, 2:3], side[:, 2:3]).astype(BF)
        seq_of = lax.broadcasted_iota(jnp.int32, (n, owners * rows), 1) // steps
        seq = lax.broadcasted_iota(jnp.int32, (n, owners * rows), 0)
        before = (seq < seq_of).astype(F32).astype(BF)
        same = (seq == seq_of).astype(F32).astype(BF)
        over = (((0,), (0,)), ((), ()))
        start = lax.dot_general(lens_all, before, over, preferred_element_type=F32)[:8]
        length = lax.dot_general(lens_all, same, over, preferred_element_type=F32)[:8]
        t = lax.rem(lax.broadcasted_iota(jnp.int32, start.shape, 1), steps).astype(F32)
        spot = jnp.where(t < length, start + t, -1.0)
        for d in range(owners):
            where_ref[d : d + 1, :] = spot[:1, d * rows : (d + 1) * rows]
    weighted = (q3 * jnp.exp(total)).reshape(rows, key_dim).astype(BF)
    load.wait()
    carried = [
        dot(weighted[s * steps : (s + 1) * steps], state[s].astype(BF)) for s in range(seqs)
    ]
    out = out.reshape(rows, value_dim) + jnp.concatenate(carried, axis=0)
    scale = lax.rsqrt(jnp.mean(out * out, axis=-1, keepdims=True) + EPS)
    silu = r / (1.0 + jnp.exp(-r))
    g_ref[...] = (out * scale * hs_ref[...].astype(F32) * silu * live[:, :1]).astype(BF)


def call_recur(layer, full_width, with_plan, owners, lens, parts, shift, extra, head_scale, state, steps):
    _, seqs, key_dim, value_dim = state.shape
    rows = seqs * steps
    blocked = lambda p: pl.BlockSpec((1, *p.shape[1:]), lambda *_: (0, 0, 0))
    ma, mb, ca, cb, ra, rb, ra2, rb2 = parts
    out_shape = [
        jax.ShapeDtypeStruct((rows, value_dim), BF),
        jax.ShapeDtypeStruct((rows, key_dim), BF),
        jax.ShapeDtypeStruct((rows, value_dim), BF),
        jax.ShapeDtypeStruct((seqs, 1, key_dim), F32),
    ]
    if with_plan:
        out_shape.append(jax.ShapeDtypeStruct((owners, rows), F32))
    return pl.pallas_call(
        functools.partial(recur, layer, full_width, with_plan, steps),
        grid_spec=pltpu.PrefetchScalarGridSpec(
            num_scalar_prefetch=1,
            grid=(1,),
            in_specs=[
                blocked(ma),
                blocked(mb),
                blocked(ca),
                blocked(cb),
                blocked(ra),
                pl.BlockSpec((1, *rb.shape[1:]), lambda *_: (1, 0, 0)),
                whole(ra2.shape),
                whole(rb2.shape),
                whole((1, key_dim)),
                whole((rows, 1)),
                whole((1, value_dim)),
                pl.BlockSpec(memory_space=pl.ANY),
            ],
            out_specs=[whole(o.shape) for o in out_shape],
            scratch_shapes=[pltpu.VMEM((seqs, key_dim, value_dim), F32), pltpu.SemaphoreType.DMA],
        ),
        out_shape=out_shape,
        compiler_params=params("arbitrary"),
        name="recur",
    )(lens, *parts, shift[layer : layer + 1], extra, head_scale[layer : layer + 1], state)


def update(steps, wk_ref, v_ref, end_ref, state_ref, *refs):
    out_ref = refs[-1]
    for s in range(state_ref.shape[1]):
        keys = wk_ref[s * steps : (s + 1) * steps, :]
        values = v_ref[s * steps : (s + 1) * steps, :]
        fresh = lax.dot_general(keys, values, (((0,), (0,)), ((), ())), preferred_element_type=F32)
        end = end_ref[s]
        keep = jnp.transpose(jnp.broadcast_to(end, (end.shape[1], end.shape[1])))[:, :1]
        out_ref[0, s] = keep * state_ref[0, s] + fresh


def call_update(layer, steps, wk, v, end, state, previous):
    layers, seqs, key_dim, value_dim = state.shape
    step_seqs = 4
    block = pl.BlockSpec((1, step_seqs, key_dim, value_dim), lambda i: (layer, i, 0, 0))
    operands = [wk, v, end, state]
    in_specs = [
        pl.BlockSpec((step_seqs * steps, key_dim), lambda i: (i, 0)),
        pl.BlockSpec((step_seqs * steps, value_dim), lambda i: (i, 0)),
        pl.BlockSpec((step_seqs, 1, key_dim), lambda i: (i, 0, 0)),
        block,
    ]
    alias = {}
    if previous is not None:
        operands.append(previous)
        in_specs.append(pl.BlockSpec(memory_space=pl.ANY))
        alias = {4: 0}
    return pl.pallas_call(
        functools.partial(update, steps),
        grid=(seqs // step_seqs,),
        in_specs=in_specs,
        out_specs=block,
        out_shape=jax.ShapeDtypeStruct(state.shape, F32),
        input_output_aliases=alias,
        compiler_params=params("arbitrary"),
        name="update_state",
    )(*operands)


def target_ids(meta, count, tp, span):
    row = lax.broadcasted_iota(jnp.int32, (count, 1), 0)
    group = row // (ROUNDS * span)
    offset = jnp.where(group == ROUNDS - 1, tp - 1, group)
    block = lax.rem(meta[8] + offset + ROUNDS * lax.rem(row // span, ROUNDS), tp)
    return (block * span + lax.rem(row, span)).astype(F32)


def close(tp, meta, where_ref, *refs):
    g_refs, (c_ref, own, plus, minus, far_a, far_b) = refs[:8], refs[8:]
    rows = where_ref.shape[1]
    count = own.shape[0] * ROUNDS
    span = count // tp
    ids = jnp.broadcast_to(target_ids(meta, count, tp, span), (count, rows))
    gathered = jnp.zeros((count, g_refs[0].shape[1]), F32)
    for i, g in enumerate(g_refs):
        chosen = (ids == where_ref[pl.ds(meta[i], 1), :]).astype(F32).astype(BF)
        gathered = gathered + dot(chosen, g[...])
    y = dot(gathered.astype(BF), c_ref[0])
    n, half = own.shape[0], far_a.shape[1]
    own[...] = y[:n]
    plus[...] = y[n : 2 * n].astype(BF)
    far_a[...] = y[2 * n : 3 * n, :half].astype(BF)
    far_b[span:, :] = y[2 * n : 3 * n - span, half:].astype(BF)
    far_b[:span, :] = y[3 * n - span : 3 * n, half:].astype(BF)
    minus[...] = y[3 * n :].astype(BF)


def call_close(layer, tp, meta, where, gs, closing, live_rows):
    width = closing.shape[2]
    n = live_rows // ROUNDS
    out_shape = [
        jax.ShapeDtypeStruct((n, width), F32),
        jax.ShapeDtypeStruct((n, width), BF),
        jax.ShapeDtypeStruct((n, width), BF),
        jax.ShapeDtypeStruct((n, width // 2), BF),
        jax.ShapeDtypeStruct((n, width // 2), BF),
    ]
    return pl.pallas_call(
        functools.partial(close, tp),
        grid_spec=pltpu.PrefetchScalarGridSpec(
            num_scalar_prefetch=1,
            grid=(1,),
            in_specs=[
                whole(where.shape),
                *(whole(g.shape) for g in gs),
                pl.BlockSpec((1, *closing.shape[1:]), lambda *_: (layer, 0, 0)),
            ],
            out_specs=[whole(o.shape) for o in out_shape],
        ),
        out_shape=out_shape,
        compiler_params=params("arbitrary"),
        name="close",
    )(meta, where, *gs, closing)


def own_rows(tp, meta, where_ref, x_ref, out_ref):
    span = out_ref.shape[0]
    rows = where_ref.shape[1]
    ids = (meta[8] * span + lax.broadcasted_iota(jnp.int32, (span, rows), 0)).astype(F32)
    total = jnp.zeros(out_ref.shape, F32)
    for d in range(where_ref.shape[0]):
        chosen = (ids == where_ref[d : d + 1, :]).astype(F32).astype(BF)
        total = total + dot(chosen, x_ref[d * rows : (d + 1) * rows, :])
    out_ref[...] = total.astype(BF)


def call_own_rows(tp, meta, where, x, live_rows):
    out = jax.ShapeDtypeStruct((live_rows // tp, x.shape[1]), BF)
    return pl.pallas_call(
        functools.partial(own_rows, tp),
        grid_spec=pltpu.PrefetchScalarGridSpec(
            num_scalar_prefetch=1,
            grid=(1,),
            in_specs=[whole(where.shape), whole(x.shape)],
            out_specs=whole(out.shape),
        ),
        out_shape=out,
        compiler_params=params("arbitrary"),
        name="own_rows",
    )(meta, where, x)


def to_chip(x, flip):
    n = lax.axis_size("dp")
    return lax.ppermute(x, "dp", [(d, 2 * ((d // 2) ^ flip) + d % 2) for d in range(n)])


def to_core(x):
    n = lax.axis_size("dp")
    return lax.ppermute(x, "dp", [(d, d ^ 1) for d in range(n)])


def along(x, step):
    n = lax.axis_size("tp")
    return lax.ppermute(x, "tp", [(i, (i + step) % n) for i in range(n)])


def dp_sum(send, mine):
    (sa, sb), (ma, mb) = send, mine
    ca, cb = to_core(sa), to_core(sb)
    ra = to_chip(ma[1:3] + ca[1:3], 1)
    rb = to_chip(mb[2:4] + cb[2:4], 3)

    def three(m, c, r):
        return (m.astype(F32) + c.astype(F32) + r.astype(F32)).astype(BF)

    ra2 = to_chip(three(ma[3], ca[3], ra[1]), 3)
    rb2 = to_chip(three(mb[1], cb[1], rb[0]), 1)
    return ma, mb, ca, cb, ra, rb, ra2, rb2


def dp_gather(g):
    near = [g, to_chip(g, 1), to_chip(g, 2), to_chip(g, 3)]
    return near + [to_core(x) for x in near]


def tp_sum(parts, x_own, tp):
    own, plus, minus, far_a, far_b = parts
    far = tp // ROUNDS
    r_p = along(plus, 1)
    r_m = along(minus, -1)
    r_a = along(far_a, 2)
    r_b = along(far_b, -2)
    total = own + r_p.astype(F32) + r_m.astype(F32) + jnp.concatenate([r_a, r_b], axis=1).astype(F32)
    total = total.reshape(ROUNDS, -1, total.shape[1])
    arrived = [along(total[j].astype(BF), ROUNDS * j) for j in range(1, far)]
    mixed = total[0]
    for a in arrived:
        mixed = mixed + a.astype(F32)
    return (x_own.astype(F32) + mixed).astype(BF)


def tp_gather(x, tp):
    far = tp // ROUNDS
    own = jnp.concatenate([x] + [along(x, ROUNDS * j) for j in range(1, far)], axis=0)
    half = own.shape[1] // 2
    plus = along(own, -1)
    minus = along(own, 1)
    far_a = along(own[:, :half], -2)
    far_b = along(own[:, half:], 2)
    return own, plus, minus, far_a, far_b


def shards(
    skip_path_activations,
    novel_lengths_per_sequence,
    input_normalizer_scales,
    question_projector,
    lookup_projector,
    payload_projector,
    emitted_valve_projector,
    keeping_valve_projector,
    keeping_valve_shift,
    additional_dwindle_exponent,
    headwise_normalizer_scales,
    closing_projector,
    earlier_recurrence_grid,
):
    streams, steps, width = skip_path_activations.shape
    dp, tp = lax.axis_size("dp"), lax.axis_size("tp")
    chips = dp // 2
    full_width = width * dp
    live_rows = streams * steps // 2
    x = skip_path_activations.reshape(streams * steps, width)
    lens = novel_lengths_per_sequence
    gain = input_normalizer_scales
    weights = (
        question_projector,
        lookup_projector,
        payload_projector,
        emitted_valve_projector,
        keeping_valve_projector,
    )
    layers, seqs, heads, key_dim, value_dim = earlier_recurrence_grid.shape
    state = earlier_recurrence_grid.reshape(layers, seqs * heads, key_dim, value_dim)
    extra = additional_dwindle_exponent.reshape(seqs * steps, 1)

    me = lax.axis_index("dp")
    slot = lax.iota(jnp.int32, 16)
    owner = 2 * ((me // 2) ^ (slot % chips)) + ((me % 2) ^ ((slot // chips) % 2))
    meta = jnp.where(slot == 8, lax.axis_index("tp"), jnp.where(slot == 9, me, owner)).astype(jnp.int32)

    new_state = None
    where = x_own = pieces = None
    for layer in range(layers):
        if layer == 0:
            run = lambda first: call_project_first(layer, first, meta, lens, x, gain, weights, chips)
        else:
            run = lambda first: call_project_next(layer, first, tp, meta, where, pieces, gain, weights, chips)
        send = run(chips)
        mine = run(0)
        parts = dp_sum(send, mine)
        out = call_recur(
            layer, full_width, layer == 0, dp, lens, parts, keeping_valve_shift, extra,
            headwise_normalizer_scales, state, steps,
        )
        if layer == 0:
            g, wk, v, end, where = out
            x_own = call_own_rows(tp, meta, where, x, live_rows)
        else:
            g, wk, v, end = out
        new_state = call_update(layer, steps, wk, v, end, state, new_state)
        sums = call_close(layer, tp, meta, where, dp_gather(g), closing_projector, live_rows)
        x_own = tp_sum(sums, x_own, tp)
        pieces = tp_gather(x_own, tp)
    stream = call_finish(tp, meta, where, pieces, x)
    return (
        stream.reshape(streams, steps, width),
        new_state.reshape(earlier_recurrence_grid.shape),
    )


def solution(mesh):
    in_specs = (
        P("grp", None, "dp"),
        P(("grp", "dp")),
        P(None, "dp"),
        P(None, "dp", "tp"),
        P(None, "dp", "tp"),
        P(None, "dp", "tp"),
        P(None, "dp", "tp"),
        P(None, "dp", "tp"),
        P(None, "tp"),
        P(("grp", "dp"), None, "tp"),
        P(),
        P(None, "tp", "dp"),
        P(None, ("grp", "dp"), "tp", None, None),
    )
    out_specs = (P("grp", None, "dp"), P(None, ("grp", "dp"), "tp", None, None))
    return jax.shard_map(shards, mesh=mesh, in_specs=in_specs, out_specs=out_specs, check_vma=False)
```

```python
import functools

import jax
import jax.numpy as jnp
from jax import lax
from jax.experimental import pallas as pl
from jax.experimental.pallas import tpu as pltpu
from jax.sharding import PartitionSpec as P

LAYERS = 2
EPS = 1e-06
TAU = 16.0
BF = jnp.bfloat16
F32 = jnp.float32
VMEM_LIMIT = 8 * 1024 * 1024
ROUNDS = 4
SIDE = 128


def dot(a, b):
    return jnp.dot(a, b, preferred_element_type=F32)


def params(*semantics):
    return pltpu.CompilerParams(vmem_limit_bytes=VMEM_LIMIT, dimension_semantics=semantics or None)


def row_of(ref, layer):
    row = ref[0:1, :]
    for i in range(1, ref.shape[0]):
        row = jnp.where(layer == i, ref[i : i + 1, :], row)
    return row


def in_hbm(x):
    return pltpu.with_memory_space_constraint(x, pltpu.MemorySpace.HBM)


def whole(shape):
    return pl.BlockSpec(shape, lambda *_: (0,) * len(shape))


def project(layer, x, gain_ref, w_refs, out_ref, lens_col):
    blocks, _, rows, _ = out_ref.shape
    xf = x.astype(F32)
    gain = row_of(gain_ref, layer).astype(F32)
    scaled = jnp.clip(xf * gain, -1e30, 1e30).astype(BF)

    def put(half, at, value):
        for j in range(blocks):
            out_ref[j, half, :, at : at + value.shape[1]] = value[j * rows : (j + 1) * rows].astype(BF)

    ends = []
    for half, group in enumerate((w_refs[:3], w_refs[3:])):
        at = 0
        for w in group:
            put(half, at, dot(scaled, w[0]))
            at += w.shape[-1]
        ends.append(at)
    squares = jnp.sum(xf * xf, axis=1, keepdims=True)
    high = squares.astype(BF).astype(F32)
    low = jnp.where(jnp.abs(high) < 3.0e38, squares - high, 0.0)
    lane = lax.broadcasted_iota(jnp.int32, (x.shape[0], SIDE), 1)
    side = jnp.where(lane == 0, high, jnp.where(lane == 1, low, 0.0))
    if lens_col is not None:
        side = jnp.where(lane == 2, lens_col, side)
    put(1, ends[1], side)


def project_first(local_seqs, meta, cfg, lens, x0, x1, x2, x3, gain_ref, wq, wk, wv, wr, wf, out_ref):
    x = jnp.concatenate([x0[...], x1[...], x2[...], x3[...]], axis=0)
    rows = x0.shape[0]
    row = lax.broadcasted_iota(jnp.int32, (rows, SIDE), 0) - meta[9] * local_seqs
    lens_col = jnp.zeros((rows, SIDE), F32)
    for s in range(local_seqs):
        lens_col = jnp.where(row == s, lens[s].astype(F32), lens_col)
    lens_col = jnp.concatenate([lens_col] * 4, axis=0)
    project(cfg[1], x, gain_ref, (wq, wk, wv, wr, wf), out_ref, lens_col)


def piece_ids(meta, shape, tp, offset):
    span = shape[1] // ROUNDS
    lane = lax.broadcasted_iota(jnp.int32, shape, 1)
    block = lax.rem(meta[8] + offset - ROUNDS * (lane // span) + 2 * tp, tp)
    return (block * span + lax.rem(lane, span)).astype(F32)


def expand(meta, tp, where_rows, pieces):
    own, plus, minus, far_a, far_b = pieces
    half = far_a.shape[1]
    rows = where_rows[0].shape[1]
    place = jnp.concatenate(
        [jnp.transpose(jnp.broadcast_to(r, (rows, rows)))[:, :1] for r in where_rows], axis=0
    )
    at = jnp.broadcast_to(place, (place.shape[0], own.shape[0]))

    def pick(offset, piece):
        chosen = (at == piece_ids(meta, at.shape, tp, offset)).astype(F32).astype(BF)
        return dot(chosen, piece)

    near = pick(0, own[...]) + pick(1, plus[...]) + pick(-1, minus[...])
    left = near[:, :half] + pick(2, far_a[...])
    right = near[:, half:] + pick(-2, far_b[...])
    return left, right, place


def project_next(tp, blocks, meta, cfg, where_ref, own, plus, minus, far_a, far_b, gain_ref, wq, wk, wv, wr, wf, out_ref):
    rows = [where_ref[pl.ds(meta[cfg[0] + j], 1), :] for j in range(blocks)]
    left, right, _ = expand(meta, tp, rows, (own, plus, minus, far_a, far_b))
    x = jnp.concatenate([left, right], axis=1)
    project(cfg[1], x, gain_ref, (wq, wk, wv, wr, wf), out_ref, None)


def finish(tp, blocks, meta, where_ref, own, plus, minus, far_a, far_b, x_ref, out_ref):
    first = pl.program_id(0) * blocks
    rows = [where_ref[pl.ds(first + j, 1), :] for j in range(blocks)]
    left, right, place = expand(meta, tp, rows, (own, plus, minus, far_a, far_b))
    half = left.shape[1]
    dead = place < 0
    out_ref[:, :half] = jnp.where(dead, x_ref[:, :half].astype(F32), left).astype(BF)
    out_ref[:, half:] = jnp.where(dead, x_ref[:, half:].astype(F32), right).astype(BF)


def weight_spec(w):
    return pl.BlockSpec((1, w.shape[1], w.shape[2]), lambda i, meta, cfg, *_: (cfg[1], 0, 0))


def projected(weights, rows, blocks):
    cols = sum(w.shape[2] for w in weights[:3])
    assert cols == sum(w.shape[2] for w in weights[3:]) + SIDE
    return jax.ShapeDtypeStruct((blocks, 2, rows, cols), BF)


def call_project_first(cfg, meta, lens, x, gain, weights, blocks):
    rows, width = x.shape[0] // (2 * blocks), x.shape[1]
    out = projected(weights, rows, blocks)

    def block_of(j):
        return pl.BlockSpec((rows, width), lambda i, meta, cfg, lens: (meta[cfg[0] + j], 0))

    return pl.pallas_call(
        functools.partial(project_first, lens.shape[0]),
        grid_spec=pltpu.PrefetchScalarGridSpec(
            num_scalar_prefetch=3,
            grid=(1,),
            in_specs=[
                *(block_of(j) for j in range(blocks)),
                whole(gain.shape),
                *(weight_spec(w) for w in weights),
            ],
            out_specs=whole(out.shape),
        ),
        out_shape=out,
        compiler_params=params("arbitrary"),
        name="project_first",
    )(meta, cfg, lens, *([in_hbm(x)] * blocks), in_hbm(gain), *(in_hbm(w) for w in weights))


def piece_specs(pieces):
    return [whole(p.shape) for p in pieces]


def call_project_next(cfg, tp, meta, where, pieces, gain, weights, blocks):
    out = projected(weights, where.shape[1], blocks)
    return pl.pallas_call(
        functools.partial(project_next, tp, blocks),
        grid_spec=pltpu.PrefetchScalarGridSpec(
            num_scalar_prefetch=2,
            grid=(1,),
            in_specs=[
                whole(where.shape),
                *piece_specs(pieces),
                whole(gain.shape),
                *(weight_spec(w) for w in weights),
            ],
            out_specs=whole(out.shape),
        ),
        out_shape=out,
        compiler_params=params("arbitrary"),
        name="project_next",
    )(meta, cfg, where, *pieces, in_hbm(gain), *weights)


def call_finish(tp, meta, where, pieces, x):
    owners, rows = where.shape
    blocks = owners // 2
    return pl.pallas_call(
        functools.partial(finish, tp, blocks),
        grid_spec=pltpu.PrefetchScalarGridSpec(
            num_scalar_prefetch=1,
            grid=(owners // blocks,),
            in_specs=[
                whole(where.shape),
                *piece_specs(pieces),
                pl.BlockSpec((blocks * rows, x.shape[1]), lambda i, *_: (i, 0)),
            ],
            out_specs=pl.BlockSpec((blocks * rows, x.shape[1]), lambda i, *_: (i, 0)),
        ),
        out_shape=jax.ShapeDtypeStruct(x.shape, BF),
        compiler_params=params("arbitrary"),
        name="finish",
    )(meta, where, *pieces, x)


def recur(full_width, steps, cfg, lens, *refs):
    (mine, core, up, down, shift_ref, extra_ref, hs_ref, state_hbm), rest = refs[:8], refs[8:]
    g_ref, wk_ref, v_ref, end_ref, where_ref, state, sem = rest
    load = pltpu.make_async_copy(state_hbm.at[cfg[1]], state, sem)
    load.start()
    seqs, key_dim, value_dim = state.shape
    rows = seqs * steps
    sum_a, sum_b = [
        (mine[0, h].astype(F32) + core[0, h].astype(F32)) + (up[h].astype(F32) + down[h].astype(F32))
        for h in range(2)
    ]
    at = value_dim + key_dim
    side = sum_b[:, at : at + SIDE]
    squares = side[:, 0:1] + side[:, 1:2]
    rms = lax.rsqrt(squares / full_width + EPS)
    q = sum_a[:, :key_dim] * (rms * key_dim ** (-0.5))
    k = sum_a[:, key_dim : 2 * key_dim] * rms
    v = sum_a[:, 2 * key_dim :] * rms
    r = sum_b[:, :value_dim] * rms
    f = sum_b[:, value_dim:at] * rms

    row = lax.broadcasted_iota(jnp.int32, (rows, key_dim), 0)
    own_len = jnp.zeros((rows, key_dim), jnp.int32)
    for s in range(seqs):
        own_len = jnp.where(row // steps == s, lens[s], own_len)
    live = jnp.where(lax.rem(row, steps) < own_len, 1.0, 0.0)
    logits = f + row_of(shift_ref, cfg[1])
    log_sig = jnp.minimum(logits, 0.0) - jnp.log(1.0 + jnp.exp(-jnp.abs(logits)))
    fade = (log_sig / TAU + extra_ref[...]) * live
    k = k * live

    def by_seq(x):
        return x.reshape(seqs, steps, x.shape[1])

    q3, k3, v3, fade3 = by_seq(q), by_seq(k), by_seq(v), by_seq(fade)
    slot = lax.broadcasted_iota(jnp.int32, (seqs, steps, key_dim), 1)
    total = jnp.zeros_like(fade3)
    for j in range(steps):
        total = total + jnp.where(slot >= j, fade3[:, j : j + 1, :], 0.0)
    out = jnp.zeros_like(v3)
    for j in range(steps):
        apart = jnp.where(slot >= j, total - total[:, j : j + 1, :], -1e30)
        score = jnp.sum(q3 * k3[:, j : j + 1, :] * jnp.exp(apart), axis=-1, keepdims=True)
        out = out + score * v3[:, j : j + 1, :]
    last = total[:, steps - 1 : steps, :]
    wk_ref[...] = (k3 * jnp.exp(last - total)).reshape(rows, key_dim).astype(BF)
    v_ref[...] = v.astype(BF)
    end_ref[...] = jnp.exp(last)
    owners = where_ref.shape[0]
    n = side.shape[0]
    lens_all = jnp.broadcast_to(side[:, 2:3], side.shape).astype(BF)
    seq_of = lax.broadcasted_iota(jnp.int32, (n, owners * rows), 1) // steps
    seq = lax.broadcasted_iota(jnp.int32, (n, owners * rows), 0)
    before = (seq < seq_of).astype(F32).astype(BF)
    same = (seq == seq_of).astype(F32).astype(BF)
    over = (((0,), (0,)), ((), ()))
    start = lax.dot_general(lens_all, before, over, preferred_element_type=F32)[:8]
    length = lax.dot_general(lens_all, same, over, preferred_element_type=F32)[:8]
    t = lax.rem(lax.broadcasted_iota(jnp.int32, start.shape, 1), steps).astype(F32)
    spot = jnp.where(t < length, start + t, -1.0)
    for d in range(owners):
        where_ref[d : d + 1, :] = spot[:1, d * rows : (d + 1) * rows]
    weighted = (q3 * jnp.exp(total)).reshape(rows, key_dim).astype(BF)
    load.wait()
    carried = [
        dot(weighted[s * steps : (s + 1) * steps], state[s].astype(BF)) for s in range(seqs)
    ]
    out = out.reshape(rows, value_dim) + jnp.concatenate(carried, axis=0)
    scale = lax.rsqrt(jnp.mean(out * out, axis=-1, keepdims=True) + EPS)
    silu = r / (1.0 + jnp.exp(-r))
    g_ref[...] = (out * scale * row_of(hs_ref, cfg[1]).astype(F32) * silu * live[:, :1]).astype(BF)


def call_recur(cfg, full_width, owners, lens, parts, shift, extra, head_scale, state, steps):
    _, seqs, key_dim, value_dim = state.shape
    rows = seqs * steps
    mine, core, up, down = parts
    first = pl.BlockSpec((1, *mine.shape[1:]), lambda *_: (0, 0, 0, 0))
    out_shape = [
        jax.ShapeDtypeStruct((rows, value_dim), BF),
        jax.ShapeDtypeStruct((rows, key_dim), BF),
        jax.ShapeDtypeStruct((rows, value_dim), BF),
        jax.ShapeDtypeStruct((seqs, 1, key_dim), F32),
        jax.ShapeDtypeStruct((owners, rows), F32),
    ]
    return pl.pallas_call(
        functools.partial(recur, full_width, steps),
        grid_spec=pltpu.PrefetchScalarGridSpec(
            num_scalar_prefetch=2,
            grid=(1,),
            in_specs=[
                first,
                first,
                whole(up.shape),
                whole(down.shape),
                whole(shift.shape),
                whole((rows, 1)),
                whole(head_scale.shape),
                pl.BlockSpec(memory_space=pltpu.MemorySpace.HBM),
            ],
            out_specs=[whole(o.shape) for o in out_shape],
            scratch_shapes=[pltpu.VMEM((seqs, key_dim, value_dim), F32), pltpu.SemaphoreType.DMA],
        ),
        out_shape=out_shape,
        compiler_params=params("arbitrary"),
        name="recur",
    )(cfg, lens, *parts, in_hbm(shift), in_hbm(extra), in_hbm(head_scale), in_hbm(state))


def update(steps, wk_ref, v_ref, end_ref, state_ref, *refs):
    out_ref = refs[-1]
    for s in range(state_ref.shape[1]):
        keys = wk_ref[s * steps : (s + 1) * steps, :]
        values = v_ref[s * steps : (s + 1) * steps, :]
        fresh = lax.dot_general(keys, values, (((0,), (0,)), ((), ())), preferred_element_type=F32)
        end = end_ref[s]
        keep = jnp.transpose(jnp.broadcast_to(end, (end.shape[1], end.shape[1])))[:, :1]
        out_ref[0, s] = keep * state_ref[0, s] + fresh


def call_update(layer, steps, wk, v, end, state, previous):
    layers, seqs, key_dim, value_dim = state.shape
    step_seqs = 4
    block = pl.BlockSpec((1, step_seqs, key_dim, value_dim), lambda i: (layer, i, 0, 0))
    operands = [wk, v, end, in_hbm(state)]
    in_specs = [
        pl.BlockSpec((step_seqs * steps, key_dim), lambda i: (i, 0)),
        pl.BlockSpec((step_seqs * steps, value_dim), lambda i: (i, 0)),
        pl.BlockSpec((step_seqs, 1, key_dim), lambda i: (i, 0, 0)),
        block,
    ]
    alias = {}
    if previous is not None:
        operands.append(previous)
        in_specs.append(pl.BlockSpec(memory_space=pl.ANY))
        alias = {4: 0}
    return pl.pallas_call(
        functools.partial(update, steps),
        grid=(seqs // step_seqs,),
        in_specs=in_specs,
        out_specs=block,
        out_shape=jax.ShapeDtypeStruct(state.shape, F32),
        input_output_aliases=alias,
        compiler_params=params("arbitrary"),
        name="update_state",
    )(*operands)


def target_ids(meta, shape, tp, span):
    row = lax.broadcasted_iota(jnp.int32, shape, 0)
    group = row // (ROUNDS * span)
    offset = jnp.where(group == ROUNDS - 1, tp - 1, group)
    block = lax.rem(meta[8] + offset + ROUNDS * lax.rem(row // span, ROUNDS), tp)
    return (block * span + lax.rem(row, span)).astype(F32)


def close(tp, meta, cfg, where_ref, *refs):
    g_refs, (c_ref, own, plus, minus, far_a, far_b) = refs[:-6], refs[-6:]
    rows = where_ref.shape[1]
    n, half = own.shape[0], far_a.shape[1]
    count = n * ROUNDS
    span = count // tp
    ids = target_ids(meta, (count, rows), tp, span)
    gathered = jnp.zeros((count, c_ref.shape[1]), F32)
    i = 0
    for g in g_refs:
        for b in range(g.shape[0]):
            chosen = (ids == where_ref[pl.ds(meta[i], 1), :]).astype(F32).astype(BF)
            gathered = gathered + dot(chosen, g[b])
            i += 1
    y = dot(gathered.astype(BF), c_ref[0])
    own[...] = y[:n]
    plus[...] = y[n : 2 * n].astype(BF)
    far_a[...] = y[2 * n : 3 * n, :half].astype(BF)
    far_b[span:, :] = y[2 * n : 3 * n - span, half:].astype(BF)
    far_b[:span, :] = y[3 * n - span : 3 * n, half:].astype(BF)
    minus[...] = y[3 * n :].astype(BF)


def call_close(cfg, tp, meta, where, gs, closing, live_rows):
    width = closing.shape[2]
    n = live_rows // ROUNDS
    out_shape = [
        jax.ShapeDtypeStruct((n, width), F32),
        jax.ShapeDtypeStruct((n, width), BF),
        jax.ShapeDtypeStruct((n, width), BF),
        jax.ShapeDtypeStruct((n, width // 2), BF),
        jax.ShapeDtypeStruct((n, width // 2), BF),
    ]
    return pl.pallas_call(
        functools.partial(close, tp),
        grid_spec=pltpu.PrefetchScalarGridSpec(
            num_scalar_prefetch=2,
            grid=(1,),
            in_specs=[
                whole(where.shape),
                *(whole(g.shape) for g in gs),
                pl.BlockSpec((1, *closing.shape[1:]), lambda i, meta, cfg: (cfg[1], 0, 0)),
            ],
            out_specs=[whole(o.shape) for o in out_shape],
        ),
        out_shape=out_shape,
        compiler_params=params("arbitrary"),
        name="close",
    )(meta, cfg, where, *gs, in_hbm(closing))


def own_rows(tp, meta, where_ref, x_ref, out_ref):
    span = out_ref.shape[0]
    rows = where_ref.shape[1]
    ids = (meta[8] * span + lax.broadcasted_iota(jnp.int32, (span, rows), 0)).astype(F32)
    total = jnp.zeros(out_ref.shape, F32)
    for d in range(where_ref.shape[0]):
        chosen = (ids == where_ref[d : d + 1, :]).astype(F32).astype(BF)
        total = total + dot(chosen, x_ref[d * rows : (d + 1) * rows, :])
    out_ref[...] = total.astype(BF)


def call_own_rows(tp, meta, where, x, live_rows):
    out = jax.ShapeDtypeStruct((live_rows // tp, x.shape[1]), BF)
    return pl.pallas_call(
        functools.partial(own_rows, tp),
        grid_spec=pltpu.PrefetchScalarGridSpec(
            num_scalar_prefetch=1,
            grid=(1,),
            in_specs=[whole(where.shape), whole(x.shape)],
            out_specs=whole(out.shape),
        ),
        out_shape=out,
        compiler_params=params("arbitrary"),
        name="own_rows",
    )(meta, where, x)


def to_chip(x, step):
    n = lax.axis_size("dp")
    return lax.ppermute(x, "dp", [(d, (d + 2 * step) % n) for d in range(n)])


def to_core(x):
    n = lax.axis_size("dp")
    return lax.ppermute(x, "dp", [(d, d ^ 1) for d in range(n)])


def along(x, step):
    n = lax.axis_size("tp")
    return lax.ppermute(x, "tp", [(i, (i + step) % n) for i in range(n)])


def dp_sum(send, mine):
    core = to_core(send)

    def both(j, h):
        return mine[j, h].astype(F32) + core[j, h].astype(F32)

    far_a = to_chip(both(2, 0).astype(BF), 1)
    far_b = to_chip(both(2, 1).astype(BF), -1)
    up = to_chip(jnp.stack([both(1, 0) + far_a.astype(F32), both(1, 1)]).astype(BF), 1)
    down = to_chip(jnp.stack([both(3, 0), both(3, 1) + far_b.astype(F32)]).astype(BF), -1)
    return mine, core, up, down


def dp_gather(g):
    own = g[None]
    core = to_core(own)
    far = to_chip(g, -2)
    rest = jnp.stack([to_chip(g, -1), far, to_chip(g, 1)])
    return own, rest, core, to_core(rest)


def tp_sum(parts, x_own, update):
    own, plus, minus, far_a, far_b = parts
    r_a = along(far_a, 2)
    r_b = along(far_b, -2)
    r_p = along(plus, 1)
    r_m = along(minus, -1)
    total = own + r_p.astype(F32) + r_m.astype(F32) + jnp.concatenate([r_a, r_b], axis=1).astype(F32)
    total = total.reshape(ROUNDS, -1, total.shape[1])
    arrived = [along(total[j].astype(BF), ROUNDS * j) for j in range(1, ROUNDS)]
    mixed, state = update(total[0])
    for a in arrived:
        mixed = mixed + a.astype(F32)
    return (x_own.astype(F32) + mixed).astype(BF), state


def tp_gather(x):
    own = jnp.concatenate([x] + [along(x, ROUNDS * j) for j in range(1, ROUNDS)], axis=0)
    half = own.shape[1] // 2
    far_a = along(own[:, :half], -2)
    far_b = along(own[:, half:], 2)
    plus = along(own, -1)
    minus = along(own, 1)
    return own, plus, minus, far_a, far_b


def shards(
    skip_path_activations,
    novel_lengths_per_sequence,
    input_normalizer_scales,
    question_projector,
    lookup_projector,
    payload_projector,
    emitted_valve_projector,
    keeping_valve_projector,
    keeping_valve_shift,
    additional_dwindle_exponent,
    headwise_normalizer_scales,
    closing_projector,
    earlier_recurrence_grid,
):
    streams, steps, width = skip_path_activations.shape
    dp, tp = lax.axis_size("dp"), lax.axis_size("tp")
    chips = dp // 2
    full_width = width * dp
    live_rows = streams * steps // 2
    x = skip_path_activations.reshape(streams * steps, width)
    lens = in_hbm(novel_lengths_per_sequence)
    gain = input_normalizer_scales
    weights = (
        question_projector,
        lookup_projector,
        payload_projector,
        emitted_valve_projector,
        keeping_valve_projector,
    )
    layers, seqs, heads, key_dim, value_dim = earlier_recurrence_grid.shape
    state = earlier_recurrence_grid.reshape(layers, seqs * heads, key_dim, value_dim)
    extra = additional_dwindle_exponent.reshape(seqs * steps, 1)

    me = lax.axis_index("dp")
    slot = lax.iota(jnp.int32, 16)
    owner = 2 * ((me // 2 + slot) % chips) + ((me % 2) ^ ((slot // chips) % 2))
    meta = jnp.where(slot == 8, lax.axis_index("tp"), jnp.where(slot == 9, me, owner)).astype(jnp.int32)

    new_state = None
    where = x_own = pieces = None
    for layer in range(layers):
        run = functools.partial(call_project_first, x=x, lens=lens)
        if layer > 0:
            run = functools.partial(call_project_next, tp=tp, where=where, pieces=pieces)
        sides = []
        for first in (chips, 0):
            cfg = in_hbm(jnp.array([first, layer], jnp.int32))
            sides.append(run(cfg, meta=meta, gain=gain, weights=weights, blocks=chips))
        parts = dp_sum(*sides)
        g, wk, v, end, spots = call_recur(
            cfg, full_width, dp, lens, parts, keeping_valve_shift, extra,
            headwise_normalizer_scales, state, steps,
        )
        if layer == 0:
            where = spots
            x_own = call_own_rows(tp, meta, where, x, live_rows)
        sums = call_close(cfg, tp, meta, where, dp_gather(g), closing_projector, live_rows)

        def update(total):
            total, keys = lax.optimization_barrier((total, wk))
            fresh = call_update(layer, steps, keys, v, end, state, new_state)
            return lax.optimization_barrier((total, fresh))

        x_own, new_state = tp_sum(sums, x_own, update)
        pieces = tp_gather(x_own)
    stream = call_finish(tp, meta, where, pieces, x)
    return (
        stream.reshape(streams, steps, width),
        new_state.reshape(earlier_recurrence_grid.shape),
    )


def solution(mesh):
    in_specs = (
        P("grp", None, "dp"),
        P(("grp", "dp")),
        P(None, "dp"),
        P(None, "dp", "tp"),
        P(None, "dp", "tp"),
        P(None, "dp", "tp"),
        P(None, "dp", "tp"),
        P(None, "dp", "tp"),
        P(None, "tp"),
        P(("grp", "dp"), None, "tp"),
        P(),
        P(None, "tp", "dp"),
        P(None, ("grp", "dp"), "tp", None, None),
    )
    out_specs = (P("grp", None, "dp"), P(None, ("grp", "dp"), "tp", None, None))
    return jax.shard_map(shards, mesh=mesh, in_specs=in_specs, out_specs=out_specs, check_vma=False)
```

```python
import functools

import jax
import jax.numpy as jnp
from jax import lax
from jax.experimental import pallas as pl
from jax.experimental.pallas import tpu as pltpu
from jax.sharding import PartitionSpec as P


EPS = 1e-06
TAU = 16.0
BF = jnp.bfloat16
F32 = jnp.float32
VMEM_LIMIT = 8 * 1024 * 1024
ROUNDS = 4
SIDE = 128


def dot(a, b):
    return jnp.dot(a, b, preferred_element_type=F32)


def params(*semantics):
    return pltpu.CompilerParams(vmem_limit_bytes=VMEM_LIMIT, dimension_semantics=semantics or None)


def row_of(ref, layer):
    row = ref[0:1, :]
    for i in range(1, ref.shape[0]):
        row = jnp.where(layer == i, ref[i : i + 1, :], row)
    return row


def in_hbm(x):
    return pltpu.with_memory_space_constraint(x, pltpu.MemorySpace.HBM)


def whole(shape):
    return pl.BlockSpec(shape, lambda *_: (0,) * len(shape))


def project(layer, x, gain_ref, w_refs, out_ref, lens_col):
    blocks, _, rows, _ = out_ref.shape
    xf = x.astype(F32)
    gain = row_of(gain_ref, layer).astype(F32)
    scaled = jnp.clip(xf * gain, -1e30, 1e30).astype(BF)

    def put(half, at, value):
        for j in range(blocks):
            out_ref[j, half, :, at : at + value.shape[1]] = value[j * rows : (j + 1) * rows].astype(BF)

    ends = []
    for half, group in enumerate((w_refs[:3], w_refs[3:])):
        at = 0
        for w in group:
            put(half, at, dot(scaled, w[0]))
            at += w.shape[-1]
        ends.append(at)
    squares = jnp.sum(xf * xf, axis=1, keepdims=True)
    high = squares.astype(BF).astype(F32)
    low = jnp.where(jnp.abs(high) < 3.0e38, squares - high, 0.0)
    lane = lax.broadcasted_iota(jnp.int32, (x.shape[0], SIDE), 1)
    side = jnp.where(lane == 0, high, jnp.where(lane == 1, low, 0.0))
    if lens_col is not None:
        side = jnp.where(lane == 2, lens_col, side)
    put(1, ends[1], side)


def project_first(layer, local_seqs, meta, lens, x0, x1, x2, x3, gain_ref, wq, wk, wv, wr, wf, out_ref):
    x = jnp.concatenate([x0[...], x1[...], x2[...], x3[...]], axis=0)
    rows = x0.shape[0]
    row = lax.broadcasted_iota(jnp.int32, (rows, SIDE), 0) - meta[9] * local_seqs
    lens_col = jnp.zeros((rows, SIDE), F32)
    for s in range(local_seqs):
        lens_col = jnp.where(row == s, lens[s].astype(F32), lens_col)
    lens_col = jnp.concatenate([lens_col] * 4, axis=0)
    project(layer, x, gain_ref, (wq, wk, wv, wr, wf), out_ref, lens_col)


def piece_ids(meta, shape, offset):
    span = shape[1] // ROUNDS
    lane = lax.broadcasted_iota(jnp.int32, shape, 1)
    block = lax.rem(meta[8] + offset + ROUNDS, ROUNDS) + ROUNDS * (lane // span)
    return (block * span + lax.rem(lane, span)).astype(F32)


def expand(meta, where_rows, pieces):
    own, plus, minus, far_a, far_b = pieces
    half = far_a.shape[1]
    rows = where_rows[0].shape[1]
    place = jnp.concatenate(
        [jnp.transpose(jnp.broadcast_to(r, (rows, rows)))[:, :1] for r in where_rows], axis=0
    )
    at = jnp.broadcast_to(place, (place.shape[0], own.shape[0]))

    def chosen(offset):
        return (at == piece_ids(meta, at.shape, offset)).astype(F32).astype(BF)

    near = dot(chosen(0), own[...]) + dot(chosen(1), plus[...]) + dot(chosen(-1), minus[...])
    far = chosen(2)
    left = near[:, :half] + dot(far, far_a[...])
    right = near[:, half:] + dot(far, far_b[...])
    return left, right, place


def project_next(layer, first, blocks, meta, where_ref, *refs):
    *pieces, gain_ref, wq, wk, wv, wr, wf, out_ref = refs
    rows = [where_ref[pl.ds(meta[first + j], 1), :] for j in range(blocks)]
    left, right, _ = expand(meta, rows, pieces)
    x = jnp.concatenate([left, right], axis=1)
    project(layer, x, gain_ref, (wq, wk, wv, wr, wf), out_ref, None)


def finish(blocks, meta, where_ref, *refs):
    *pieces, x_ref, out_ref = refs
    first = pl.program_id(0) * blocks
    rows = [where_ref[pl.ds(first + j, 1), :] for j in range(blocks)]
    left, right, place = expand(meta, rows, pieces)
    half = left.shape[1]
    dead = place < 0
    out_ref[:, :half] = jnp.where(dead, x_ref[:, :half].astype(F32), left).astype(BF)
    out_ref[:, half:] = jnp.where(dead, x_ref[:, half:].astype(F32), right).astype(BF)


def weight_spec(layer, w):
    return pl.BlockSpec((1, w.shape[1], w.shape[2]), lambda *_: (layer, 0, 0))


def projected(weights, rows, blocks):
    cols = sum(w.shape[2] for w in weights[:3])
    assert cols == sum(w.shape[2] for w in weights[3:]) + SIDE
    return jax.ShapeDtypeStruct((blocks, 2, rows, cols), BF)


def call_project_first(layer, first, meta, lens, x, gain, weights, blocks):
    rows, width = x.shape[0] // (2 * blocks), x.shape[1]
    out = projected(weights, rows, blocks)

    def block_of(j):
        return pl.BlockSpec((rows, width), lambda i, meta, lens: (meta[first + j], 0))

    return pl.pallas_call(
        functools.partial(project_first, layer, lens.shape[0]),
        grid_spec=pltpu.PrefetchScalarGridSpec(
            num_scalar_prefetch=2,
            grid=(1,),
            in_specs=[
                *(block_of(j) for j in range(blocks)),
                whole(gain.shape),
                *(weight_spec(layer, w) for w in weights),
            ],
            out_specs=whole(out.shape),
        ),
        out_shape=out,
        compiler_params=params("arbitrary"),
        name="project_first",
    )(meta, lens, *([in_hbm(x)] * blocks), in_hbm(gain), *(in_hbm(w) for w in weights))


def piece_specs(pieces):
    return [whole(p.shape) for p in pieces]


def call_project_next(layer, first, meta, where, pieces, gain, weights, blocks):
    out = projected(weights, where.shape[1], blocks)
    return pl.pallas_call(
        functools.partial(project_next, layer, first, blocks),
        grid_spec=pltpu.PrefetchScalarGridSpec(
            num_scalar_prefetch=1,
            grid=(1,),
            in_specs=[
                whole(where.shape),
                *piece_specs(pieces),
                whole(gain.shape),
                *(weight_spec(layer, w) for w in weights),
            ],
            out_specs=whole(out.shape),
        ),
        out_shape=out,
        compiler_params=params("arbitrary"),
        name="project_next",
    )(meta, where, *pieces, gain, *weights)


def call_finish(meta, where, pieces, x):
    owners, rows = where.shape
    blocks = owners // 2
    return pl.pallas_call(
        functools.partial(finish, blocks),
        grid_spec=pltpu.PrefetchScalarGridSpec(
            num_scalar_prefetch=1,
            grid=(owners // blocks,),
            in_specs=[
                whole(where.shape),
                *piece_specs(pieces),
                pl.BlockSpec((blocks * rows, x.shape[1]), lambda i, *_: (i, 0)),
            ],
            out_specs=pl.BlockSpec((blocks * rows, x.shape[1]), lambda i, *_: (i, 0)),
        ),
        out_shape=jax.ShapeDtypeStruct(x.shape, BF),
        compiler_params=params("arbitrary"),
        name="finish",
    )(meta, where, *pieces, x)


def recur(layer, full_width, steps, lens, *refs):
    (mine, core, up, down, shift_ref, extra_ref, hs_ref, state), rest = refs[:8], refs[8:]
    g_ref, wk_ref, v_ref, end_ref = rest[:4]
    seqs, key_dim, value_dim = state.shape
    rows = seqs * steps
    sum_a, sum_b = [
        (mine[0, h].astype(F32) + core[0, h].astype(F32)) + (up[h].astype(F32) + down[h].astype(F32))
        for h in range(2)
    ]
    at = value_dim + key_dim
    side = sum_b[:, at : at + SIDE]
    squares = side[:, 0:1] + side[:, 1:2]
    rms = lax.rsqrt(squares / full_width + EPS)
    q = sum_a[:, :key_dim] * (rms * key_dim ** (-0.5))
    k = sum_a[:, key_dim : 2 * key_dim] * rms
    v = sum_a[:, 2 * key_dim :] * rms
    r = sum_b[:, :value_dim] * rms
    f = sum_b[:, value_dim:at] * rms

    row = lax.broadcasted_iota(jnp.int32, (rows, key_dim), 0)
    own_len = jnp.zeros((rows, key_dim), jnp.int32)
    for s in range(seqs):
        own_len = jnp.where(row // steps == s, lens[s], own_len)
    live = jnp.where(lax.rem(row, steps) < own_len, 1.0, 0.0)
    logits = f + row_of(shift_ref, layer)
    log_sig = jnp.minimum(logits, 0.0) - jnp.log(1.0 + jnp.exp(-jnp.abs(logits)))
    fade = (log_sig / TAU + extra_ref[...]) * live
    k = k * live

    def by_seq(x):
        return x.reshape(seqs, steps, x.shape[1])

    q3, k3, v3, fade3 = by_seq(q), by_seq(k), by_seq(v), by_seq(fade)
    slot = lax.broadcasted_iota(jnp.int32, (seqs, steps, key_dim), 1)
    total = jnp.zeros_like(fade3)
    for j in range(steps):
        total = total + jnp.where(slot >= j, fade3[:, j : j + 1, :], 0.0)
    out = jnp.zeros_like(v3)
    for j in range(steps):
        apart = jnp.where(slot >= j, total - total[:, j : j + 1, :], -1e30)
        score = jnp.sum(q3 * k3[:, j : j + 1, :] * jnp.exp(apart), axis=-1, keepdims=True)
        out = out + score * v3[:, j : j + 1, :]
    last = total[:, steps - 1 : steps, :]
    wk_ref[...] = (k3 * jnp.exp(last - total)).reshape(rows, key_dim).astype(BF)
    v_ref[...] = v.astype(BF)
    end_ref[...] = jnp.exp(last)
    for where_ref in rest[4:]:
        owners = where_ref.shape[0]
        n = side.shape[0]
        lens_all = jnp.broadcast_to(side[:, 2:3], side.shape).astype(BF)
        seq_of = lax.broadcasted_iota(jnp.int32, (n, owners * rows), 1) // steps
        seq = lax.broadcasted_iota(jnp.int32, (n, owners * rows), 0)
        before = (seq < seq_of).astype(F32).astype(BF)
        same = (seq == seq_of).astype(F32).astype(BF)
        over = (((0,), (0,)), ((), ()))
        start = lax.dot_general(lens_all, before, over, preferred_element_type=F32)[:8]
        length = lax.dot_general(lens_all, same, over, preferred_element_type=F32)[:8]
        t = lax.rem(lax.broadcasted_iota(jnp.int32, start.shape, 1), steps).astype(F32)
        spot = jnp.where(t < length, start + t, -1.0)
        for d in range(owners):
            where_ref[d : d + 1, :] = spot[:1, d * rows : (d + 1) * rows]
    weighted = (q3 * jnp.exp(total)).reshape(rows, key_dim).astype(BF)
    carried = [
        dot(weighted[s * steps : (s + 1) * steps], state[s].astype(BF)) for s in range(seqs)
    ]
    out = out.reshape(rows, value_dim) + jnp.concatenate(carried, axis=0)
    scale = lax.rsqrt(jnp.mean(out * out, axis=-1, keepdims=True) + EPS)
    silu = r / (1.0 + jnp.exp(-r))
    g_ref[...] = (out * scale * row_of(hs_ref, layer).astype(F32) * silu * live[:, :1]).astype(BF)


def call_recur(layer, full_width, owners, lens, parts, shift, extra, head_scale, state, steps):
    seqs, key_dim, value_dim = state.shape
    rows = seqs * steps
    mine, _, up, down = parts
    first = pl.BlockSpec((1, *mine.shape[1:]), lambda *_: (0, 0, 0, 0))
    out_shape = [
        jax.ShapeDtypeStruct((rows, value_dim), BF),
        jax.ShapeDtypeStruct((rows, key_dim), BF),
        jax.ShapeDtypeStruct((rows, value_dim), BF),
        jax.ShapeDtypeStruct((seqs, 1, key_dim), F32),
    ]
    if layer == 0:
        out_shape.append(jax.ShapeDtypeStruct((owners, rows), F32))
    return pl.pallas_call(
        functools.partial(recur, layer, full_width, steps),
        grid_spec=pltpu.PrefetchScalarGridSpec(
            num_scalar_prefetch=1,
            grid=(1,),
            in_specs=[
                first,
                first,
                whole(up.shape),
                whole(down.shape),
                whole(shift.shape),
                whole((rows, 1)),
                whole(head_scale.shape),
                whole(state.shape),
            ],
            out_specs=[whole(o.shape) for o in out_shape],
        ),
        out_shape=out_shape,
        compiler_params=params("arbitrary"),
        name="recur",
    )(lens, *parts, shift, extra, head_scale, state)


def load(layer, after_ref, state_hbm, out_ref, sem):
    copy = pltpu.make_async_copy(state_hbm.at[layer], out_ref, sem)
    copy.start()
    copy.wait()


def call_load(layer, after, state):
    return pl.pallas_call(
        functools.partial(load, layer),
        grid=(1,),
        in_specs=[whole(after.shape), pl.BlockSpec(memory_space=pltpu.MemorySpace.HBM)],
        out_specs=pl.BlockSpec(memory_space=pltpu.MemorySpace.VMEM),
        out_shape=pltpu.VMEM(state.shape[1:], F32),
        scratch_shapes=[pltpu.SemaphoreType.DMA],
        compiler_params=params("arbitrary"),
        name="load_state",
    )(after, in_hbm(state))


def update(steps, wk_ref, v_ref, end_ref, state_ref, *refs):
    out_ref = refs[-1]
    for s in range(state_ref.shape[0]):
        keys = wk_ref[s * steps : (s + 1) * steps, :]
        values = v_ref[s * steps : (s + 1) * steps, :]
        fresh = lax.dot_general(keys, values, (((0,), (0,)), ((), ())), preferred_element_type=F32)
        end = end_ref[s]
        keep = jnp.transpose(jnp.broadcast_to(end, (end.shape[1], end.shape[1])))[:, :1]
        out_ref[0, s] = keep * state_ref[s] + fresh


def call_update(layer, layers, steps, wk, v, end, state, previous):
    seqs, key_dim, value_dim = state.shape
    step_seqs = 4
    block = pl.BlockSpec((1, step_seqs, key_dim, value_dim), lambda i: (layer, i, 0, 0))
    operands = [wk, v, end, state]
    in_specs = [
        pl.BlockSpec((step_seqs * steps, key_dim), lambda i: (i, 0)),
        pl.BlockSpec((step_seqs * steps, value_dim), lambda i: (i, 0)),
        pl.BlockSpec((step_seqs, 1, key_dim), lambda i: (i, 0, 0)),
        pl.BlockSpec((step_seqs, key_dim, value_dim), lambda i: (i, 0, 0)),
    ]
    alias = {}
    if previous is not None:
        operands.append(previous)
        in_specs.append(pl.BlockSpec(memory_space=pl.ANY))
        alias = {4: 0}
    return pl.pallas_call(
        functools.partial(update, steps),
        grid=(seqs // step_seqs,),
        in_specs=in_specs,
        out_specs=block,
        out_shape=jax.ShapeDtypeStruct((layers, *state.shape), F32),
        input_output_aliases=alias,
        compiler_params=params("arbitrary"),
        name="update_state",
    )(*operands)


def target_ids(meta, shape, span):
    row = lax.broadcasted_iota(jnp.int32, shape, 0)
    block = lax.rem(meta[8] + row // (ROUNDS * span), ROUNDS) + ROUNDS * lax.rem(row // span, ROUNDS)
    return (block * span + lax.rem(row, span)).astype(F32)


def close(tp, meta, where_ref, *refs):
    *g_refs, c_ref, own, plus, minus, far_a, far_b = refs
    rows = where_ref.shape[1]
    n, half = far_a.shape
    count = n * ROUNDS
    span = count // tp
    ids = target_ids(meta, (count, rows), span)
    gathered = jnp.zeros((count, c_ref.shape[1]), F32)
    i = 0
    for g in g_refs:
        for b in range(g.shape[0]):
            chosen = (ids == where_ref[pl.ds(meta[i], 1), :]).astype(F32).astype(BF)
            gathered = gathered + dot(chosen, g[b])
            i += 1
    y = dot(gathered.astype(BF), c_ref[0])
    own[...] = y[:n]
    plus[...] = y[n : 2 * n].astype(BF)
    far_a[...] = y[2 * n : 3 * n, :half].astype(BF)
    far_b[...] = y[2 * n : 3 * n, half:].astype(BF)
    minus[...] = y[3 * n :].astype(BF)


def call_close(layer, tp, meta, where, gs, closing, live_rows):
    width = closing.shape[2]
    n = live_rows // ROUNDS
    out_shape = [
        jax.ShapeDtypeStruct((n, width), F32),
        jax.ShapeDtypeStruct((n, width), BF),
        jax.ShapeDtypeStruct((n, width), BF),
        jax.ShapeDtypeStruct((n, width // 2), BF),
        jax.ShapeDtypeStruct((n, width // 2), BF),
    ]
    return pl.pallas_call(
        functools.partial(close, tp),
        grid_spec=pltpu.PrefetchScalarGridSpec(
            num_scalar_prefetch=1,
            grid=(1,),
            in_specs=[
                whole(where.shape),
                *(whole(g.shape) for g in gs),
                pl.BlockSpec((1, *closing.shape[1:]), lambda *_: (layer, 0, 0)),
            ],
            out_specs=[whole(o.shape) for o in out_shape],
        ),
        out_shape=out_shape,
        compiler_params=params("arbitrary"),
        name="close",
    )(meta, where, *gs, closing)


def own_rows(span, meta, where_ref, x_ref, out_ref):
    rows = where_ref.shape[1]
    ids = target_ids(meta, (out_ref.shape[0], rows), span)
    total = jnp.zeros(out_ref.shape, F32)
    for d in range(where_ref.shape[0]):
        chosen = (ids == where_ref[d : d + 1, :]).astype(F32).astype(BF)
        total = total + dot(chosen, x_ref[d * rows : (d + 1) * rows, :])
    out_ref[...] = total.astype(BF)


def call_own_rows(tp, meta, where, x, live_rows):
    out = jax.ShapeDtypeStruct((live_rows // ROUNDS, x.shape[1]), BF)
    return pl.pallas_call(
        functools.partial(own_rows, live_rows // tp),
        grid_spec=pltpu.PrefetchScalarGridSpec(
            num_scalar_prefetch=1,
            grid=(1,),
            in_specs=[whole(where.shape), whole(x.shape)],
            out_specs=whole(out.shape),
        ),
        out_shape=out,
        compiler_params=params("arbitrary"),
        name="own_rows",
    )(meta, where, x)


def to_chip(x, step):
    n = lax.axis_size("dp")
    return lax.ppermute(x, "dp", [(d, (d + 2 * step) % n) for d in range(n)])


def to_core(x):
    n = lax.axis_size("dp")
    return lax.ppermute(x, "dp", [(d, d ^ 1) for d in range(n)])


def along(x, step):
    n = lax.axis_size("tp")
    return lax.ppermute(x, "tp", [(i, (i + step) % n) for i in range(n)])


def across(x, flip):
    n = lax.axis_size("tp")
    return lax.ppermute(x, "tp", [(i, ROUNDS * ((i // ROUNDS) ^ flip) + i % ROUNDS) for i in range(n)])


def dp_sum(send, mine, fetch):
    core = to_core(send)

    def both(j, h):
        return mine[j, h].astype(F32) + core[j, h].astype(F32)

    far_a = to_chip(both(2, 0).astype(BF), 1)
    far_b = to_chip(both(2, 1).astype(BF), -1)
    up = jnp.stack([both(1, 0) + far_a.astype(F32), both(1, 1)]).astype(BF)
    down = jnp.stack([both(3, 0), both(3, 1) + far_b.astype(F32)]).astype(BF)
    state = fetch(far_b[:8, :128])
    up, down = to_chip(up, 1), to_chip(down, -1)
    up, state = lax.optimization_barrier((up, state))
    return (mine, core, up, down), state


def dp_gather(g):
    own = g[None]
    core = to_core(own)
    far = to_chip(g, -2)
    rest = jnp.stack([to_chip(g, -1), far, to_chip(g, 1)])
    return own, rest, core, to_core(rest)


def tp_sum(parts, x_own, update):
    own, plus, minus, far_a, far_b = parts
    r_a = along(far_a, 2)
    r_b = along(far_b, -2)
    total = own + jnp.concatenate([r_a, r_b], axis=1).astype(F32)
    total = total + along(plus, 1).astype(F32) + along(minus, -1).astype(F32)
    total = total.astype(BF)
    half = total.shape[1] // 2
    left, right = total[:, :half], total[:, half:]

    def add(a, b):
        return (a.astype(F32) + b.astype(F32)).astype(BF)

    x_own, total, state = update(x_own, total)
    got_left, got_right = across(left, 1), across(right, 3)
    got_left, x_own = lax.optimization_barrier((got_left, x_own))
    left, right = add(left, got_left), add(right, got_right)
    got_left, got_right = across(left, 3), across(right, 1)
    mixed = jnp.concatenate(
        [left.astype(F32) + got_left.astype(F32), right.astype(F32) + got_right.astype(F32)], axis=1
    )
    return (x_own.astype(F32) + mixed).astype(BF), state


def tp_gather(own):
    half = own.shape[1] // 2
    far_a = along(own[:, :half], -2)
    far_b = along(own[:, half:], 2)
    plus = along(own, -1)
    minus = along(own, 1)
    return own, plus, minus, far_a, far_b


def shards(
    skip_path_activations,
    novel_lengths_per_sequence,
    input_normalizer_scales,
    question_projector,
    lookup_projector,
    payload_projector,
    emitted_valve_projector,
    keeping_valve_projector,
    keeping_valve_shift,
    additional_dwindle_exponent,
    headwise_normalizer_scales,
    closing_projector,
    earlier_recurrence_grid,
):
    streams, steps, width = skip_path_activations.shape
    dp, tp = lax.axis_size("dp"), lax.axis_size("tp")
    chips = dp // 2
    full_width = width * dp
    live_rows = streams * steps // 2
    x = skip_path_activations.reshape(streams * steps, width)
    lens = novel_lengths_per_sequence
    gain = input_normalizer_scales
    weights = (
        question_projector,
        lookup_projector,
        payload_projector,
        emitted_valve_projector,
        keeping_valve_projector,
    )
    layers, seqs, heads, key_dim, value_dim = earlier_recurrence_grid.shape
    state = earlier_recurrence_grid.reshape(layers, seqs * heads, key_dim, value_dim)
    extra = additional_dwindle_exponent.reshape(seqs * steps, 1)

    me = lax.axis_index("dp")
    slot = lax.iota(jnp.int32, 16)
    owner = 2 * ((me // 2 + slot) % chips) + ((me % 2) ^ ((slot // chips) % 2))
    meta = jnp.where(slot == 8, lax.axis_index("tp"), jnp.where(slot == 9, me, owner)).astype(jnp.int32)

    new_state = None
    where = x_own = pieces = None
    for layer in range(layers):
        if layer == 0:
            run = lambda first: call_project_first(layer, first, meta, lens, x, gain, weights, chips)
        else:
            run = lambda first: call_project_next(layer, first, meta, where, pieces, gain, weights, chips)
        send = run(chips)
        mine = run(0)
        parts, held = dp_sum(send, mine, lambda after: call_load(layer, after, state))
        g, wk, v, end, *spots = call_recur(
            layer, full_width, dp, lens, parts, keeping_valve_shift, extra,
            headwise_normalizer_scales, held, steps,
        )
        if layer == 0:
            (where,) = spots
            x_own = call_own_rows(tp, meta, where, x, live_rows)
        sums = call_close(layer, tp, meta, where, dp_gather(g), closing_projector, live_rows)

        def update(own, total):
            total, keys = lax.optimization_barrier((total, wk))
            fresh = call_update(layer, layers, steps, keys, v, end, held, new_state)
            own, fresh = lax.optimization_barrier((own, fresh))
            return own, total, fresh

        x_own, new_state = tp_sum(sums, x_own, update)
        pieces = tp_gather(x_own)
    stream = call_finish(meta, where, pieces, x)
    return (
        stream.reshape(streams, steps, width),
        new_state.reshape(earlier_recurrence_grid.shape),
    )


def solution(mesh):
    in_specs = (
        P("grp", None, "dp"),
        P(("grp", "dp")),
        P(None, "dp"),
        P(None, "dp", "tp"),
        P(None, "dp", "tp"),
        P(None, "dp", "tp"),
        P(None, "dp", "tp"),
        P(None, "dp", "tp"),
        P(None, "tp"),
        P(("grp", "dp"), None, "tp"),
        P(),
        P(None, "tp", "dp"),
        P(None, ("grp", "dp"), "tp", None, None),
    )
    out_specs = (P("grp", None, "dp"), P(None, ("grp", "dp"), "tp", None, None))
    return jax.shard_map(shards, mesh=mesh, in_specs=in_specs, out_specs=out_specs, check_vma=False)
```

```python
import functools

import jax
import jax.numpy as jnp
from jax import lax
from jax.experimental import pallas as pl
from jax.experimental.pallas import tpu as pltpu
from jax.sharding import PartitionSpec as P


EPS = 1e-06
TAU = 16.0
BF = jnp.bfloat16
F32 = jnp.float32
VMEM_LIMIT = 8 * 1024 * 1024
ROUNDS = 4
SIDE = 128


def dot(a, b):
    return jnp.dot(a, b, preferred_element_type=F32)


def params(*semantics):
    return pltpu.CompilerParams(vmem_limit_bytes=VMEM_LIMIT, dimension_semantics=semantics or None)


def row_of(ref, layer):
    row = ref[0:1, :]
    for i in range(1, ref.shape[0]):
        row = jnp.where(layer == i, ref[i : i + 1, :], row)
    return row


def in_hbm(x):
    return pltpu.with_memory_space_constraint(x, pltpu.MemorySpace.HBM)


def whole(shape):
    return pl.BlockSpec(shape, lambda *_: (0,) * len(shape))


def project(layer, x, gain_ref, w_refs, out_ref, lens_col):
    blocks, _, rows, _ = out_ref.shape
    xf = x.astype(F32)
    gain = row_of(gain_ref, layer).astype(F32)
    scaled = jnp.clip(xf * gain, -1e30, 1e30).astype(BF)

    def put(half, at, value):
        for j in range(blocks):
            out_ref[j, half, :, at : at + value.shape[1]] = value[j * rows : (j + 1) * rows].astype(BF)

    ends = []
    for half, group in enumerate((w_refs[:3], w_refs[3:])):
        at = 0
        for w in group:
            put(half, at, dot(scaled, w[0]))
            at += w.shape[-1]
        ends.append(at)
    squares = jnp.sum(xf * xf, axis=1, keepdims=True)
    high = squares.astype(BF).astype(F32)
    low = jnp.where(jnp.abs(high) < 3.0e38, squares - high, 0.0)
    lane = lax.broadcasted_iota(jnp.int32, (x.shape[0], SIDE), 1)
    side = jnp.where(lane == 0, high, jnp.where(lane == 1, low, 0.0))
    if lens_col is not None:
        side = jnp.where(lane == 2, lens_col, side)
    put(1, ends[1], side)


def project_first(layer, local_seqs, meta, lens, x0, x1, gain_ref, wq, wk, wv, wr, wf, out_ref):
    x = jnp.concatenate([x0[...], x1[...]], axis=0)
    rows = x0.shape[0]
    row = lax.broadcasted_iota(jnp.int32, (rows, SIDE), 0) - meta[9] * local_seqs
    lens_col = jnp.zeros((rows, SIDE), F32)
    for s in range(local_seqs):
        lens_col = jnp.where(row == s, lens[s].astype(F32), lens_col)
    lens_col = jnp.concatenate([lens_col] * 2, axis=0)
    project(layer, x, gain_ref, (wq, wk, wv, wr, wf), out_ref, lens_col)


def piece_ids(meta, shape, offset):
    span = shape[1] // ROUNDS
    lane = lax.broadcasted_iota(jnp.int32, shape, 1)
    block = lax.rem(meta[8] + offset + ROUNDS, ROUNDS) + ROUNDS * (lane // span)
    return (block * span + lax.rem(lane, span)).astype(F32)


def expand(meta, where_rows, pieces):
    own, plus, minus, far = pieces
    rows = where_rows[0].shape[1]
    place = jnp.concatenate(
        [jnp.transpose(jnp.broadcast_to(r, (rows, rows)))[:, :1] for r in where_rows], axis=0
    )
    at = jnp.broadcast_to(place, (place.shape[0], own.shape[0]))

    def chosen(offset):
        return (at == piece_ids(meta, at.shape, offset)).astype(F32).astype(BF)

    x = dot(chosen(0), own[...]) + dot(chosen(1), plus[...]) + dot(chosen(-1), minus[...])
    return x + dot(chosen(2), far[...]), place


def project_next(layer, meta, where_ref, *refs):
    *pieces, gain_ref, wq, wk, wv, wr, wf, out_ref = refs
    rows = [where_ref[pl.ds(meta[j], 1), :] for j in range(out_ref.shape[0])]
    x, _ = expand(meta, rows, pieces)
    project(layer, x, gain_ref, (wq, wk, wv, wr, wf), out_ref, None)


def finish(blocks, meta, where_ref, *refs):
    *pieces, x_ref, out_ref = refs
    first = pl.program_id(0) * blocks
    rows = [where_ref[pl.ds(first + j, 1), :] for j in range(blocks)]
    live, place = expand(meta, rows, pieces)
    out_ref[...] = jnp.where(place < 0, x_ref[...].astype(F32), live).astype(BF)


def weight_spec(layer, w):
    return pl.BlockSpec((1, w.shape[1], w.shape[2]), lambda *_: (layer, 0, 0))


def projected(weights, rows, blocks):
    cols = sum(w.shape[2] for w in weights[:3])
    assert cols == sum(w.shape[2] for w in weights[3:]) + SIDE
    return jax.ShapeDtypeStruct((blocks, 2, rows, cols), BF)


def call_project_first(layer, meta, lens, x, gain, weights, blocks):
    rows, width = x.shape[0] // (2 * blocks), x.shape[1]
    out = projected(weights, rows, blocks)

    def block_of(j):
        return pl.BlockSpec((rows, width), lambda i, meta, lens: (meta[2 * i + j], 0))

    return pl.pallas_call(
        functools.partial(project_first, layer, lens.shape[0]),
        grid_spec=pltpu.PrefetchScalarGridSpec(
            num_scalar_prefetch=2,
            grid=(blocks // 2,),
            in_specs=[
                *(block_of(j) for j in range(2)),
                whole(gain.shape),
                *(weight_spec(layer, w) for w in weights),
            ],
            out_specs=pl.BlockSpec((2, *out.shape[1:]), lambda i, *_: (i, 0, 0, 0)),
        ),
        out_shape=out,
        compiler_params=params("arbitrary"),
        name="project_first",
    )(meta, lens, *([in_hbm(x)] * 2), in_hbm(gain), *(in_hbm(w) for w in weights))


def piece_specs(pieces):
    return [whole(p.shape) for p in pieces]


def call_project_next(layer, meta, where, pieces, gain, weights, blocks):
    out = projected(weights, where.shape[1], blocks)
    return pl.pallas_call(
        functools.partial(project_next, layer),
        grid_spec=pltpu.PrefetchScalarGridSpec(
            num_scalar_prefetch=1,
            grid=(1,),
            in_specs=[
                whole(where.shape),
                *piece_specs(pieces),
                whole(gain.shape),
                *(weight_spec(layer, w) for w in weights),
            ],
            out_specs=whole(out.shape),
        ),
        out_shape=out,
        compiler_params=params("arbitrary"),
        name="project_next",
    )(meta, where, *pieces, gain, *weights)


def call_finish(meta, where, pieces, x):
    owners, rows = where.shape
    blocks = owners // 2
    return pl.pallas_call(
        functools.partial(finish, blocks),
        grid_spec=pltpu.PrefetchScalarGridSpec(
            num_scalar_prefetch=1,
            grid=(owners // blocks,),
            in_specs=[
                whole(where.shape),
                *piece_specs(pieces),
                pl.BlockSpec((blocks * rows, x.shape[1]), lambda i, *_: (i, 0)),
            ],
            out_specs=pl.BlockSpec((blocks * rows, x.shape[1]), lambda i, *_: (i, 0)),
        ),
        out_shape=jax.ShapeDtypeStruct(x.shape, BF),
        compiler_params=params("arbitrary"),
        name="finish",
    )(meta, where, *pieces, x)


def recur(full_width, steps, meta, lens, *refs):
    layer = meta[10]
    (mine, core, up, down, shift_ref, extra_ref, hs_ref, state), rest = refs[:8], refs[8:]
    g_ref, wk_ref, v_ref, end_ref, side_ref = rest
    seqs, key_dim, value_dim = state.shape
    rows = seqs * steps
    sum_a, sum_b = [
        (mine[0, h].astype(F32) + core[0, h].astype(F32)) + (up[h].astype(F32) + down[h].astype(F32))
        for h in range(2)
    ]
    at = value_dim + key_dim
    side = sum_b[:, at : at + SIDE]
    squares = side[:, 0:1] + side[:, 1:2]
    rms = lax.rsqrt(squares / full_width + EPS)
    q = sum_a[:, :key_dim] * (rms * key_dim ** (-0.5))
    k = sum_a[:, key_dim : 2 * key_dim] * rms
    v = sum_a[:, 2 * key_dim :] * rms
    r = sum_b[:, :value_dim] * rms
    f = sum_b[:, value_dim:at] * rms

    row = lax.broadcasted_iota(jnp.int32, (rows, key_dim), 0)
    own_len = jnp.zeros((rows, key_dim), jnp.int32)
    for s in range(seqs):
        own_len = jnp.where(row // steps == s, lens[s], own_len)
    live = jnp.where(lax.rem(row, steps) < own_len, 1.0, 0.0)
    logits = f + row_of(shift_ref, layer)
    log_sig = jnp.minimum(logits, 0.0) - jnp.log(1.0 + jnp.exp(-jnp.abs(logits)))
    fade = (log_sig / TAU + extra_ref[...]) * live
    k = k * live

    def by_seq(x):
        return x.reshape(seqs, steps, x.shape[1])

    q3, k3, v3, fade3 = by_seq(q), by_seq(k), by_seq(v), by_seq(fade)
    slot = lax.broadcasted_iota(jnp.int32, (seqs, steps, key_dim), 1)
    total = jnp.zeros_like(fade3)
    for j in range(steps):
        total = total + jnp.where(slot >= j, fade3[:, j : j + 1, :], 0.0)
    out = jnp.zeros_like(v3)
    for j in range(steps):
        apart = jnp.where(slot >= j, total - total[:, j : j + 1, :], -1e30)
        score = jnp.sum(q3 * k3[:, j : j + 1, :] * jnp.exp(apart), axis=-1, keepdims=True)
        out = out + score * v3[:, j : j + 1, :]
    last = total[:, steps - 1 : steps, :]
    wk_ref[...] = (k3 * jnp.exp(last - total)).reshape(rows, key_dim).astype(BF)
    v_ref[...] = v.astype(BF)
    end_ref[...] = jnp.exp(last)
    side_ref[...] = side
    weighted = (q3 * jnp.exp(total)).reshape(rows, key_dim).astype(BF)
    carried = [
        dot(weighted[s * steps : (s + 1) * steps], state[s].astype(BF)) for s in range(seqs)
    ]
    out = out.reshape(rows, value_dim) + jnp.concatenate(carried, axis=0)
    scale = lax.rsqrt(jnp.mean(out * out, axis=-1, keepdims=True) + EPS)
    silu = r / (1.0 + jnp.exp(-r))
    g_ref[...] = (out * scale * row_of(hs_ref, layer).astype(F32) * silu * live[:, :1]).astype(BF)


def call_recur(meta, full_width, lens, parts, shift, extra, head_scale, state, steps):
    seqs, key_dim, value_dim = state.shape
    rows = seqs * steps
    mine, _, up, down = parts
    first = pl.BlockSpec((1, *mine.shape[1:]), lambda *_: (0, 0, 0, 0))
    out_shape = [
        jax.ShapeDtypeStruct((rows, value_dim), BF),
        jax.ShapeDtypeStruct((rows, key_dim), BF),
        jax.ShapeDtypeStruct((rows, value_dim), BF),
        jax.ShapeDtypeStruct((seqs, 1, key_dim), F32),
        jax.ShapeDtypeStruct((rows, SIDE), F32),
    ]
    return pl.pallas_call(
        functools.partial(recur, full_width, steps),
        grid_spec=pltpu.PrefetchScalarGridSpec(
            num_scalar_prefetch=2,
            grid=(1,),
            in_specs=[
                first,
                first,
                whole(up.shape),
                whole(down.shape),
                whole(shift.shape),
                whole((rows, 1)),
                whole(head_scale.shape),
                whole(state.shape),
            ],
            out_specs=[whole(o.shape) for o in out_shape],
        ),
        out_shape=out_shape,
        compiler_params=params("arbitrary"),
        name="recur",
    )(meta, lens, *parts, shift, extra, head_scale, state)


def plan(steps, side_ref, where_ref):
    side = side_ref[...]
    rows = where_ref.shape[1]
    owners = where_ref.shape[0]
    n = side.shape[0]
    lens_all = jnp.broadcast_to(side[:, 2:3], side.shape).astype(BF)
    seq_of = lax.broadcasted_iota(jnp.int32, (n, owners * rows), 1) // steps
    seq = lax.broadcasted_iota(jnp.int32, (n, owners * rows), 0)
    before = (seq < seq_of).astype(F32).astype(BF)
    same = (seq == seq_of).astype(F32).astype(BF)
    over = (((0,), (0,)), ((), ()))
    start = lax.dot_general(lens_all, before, over, preferred_element_type=F32)[:8]
    length = lax.dot_general(lens_all, same, over, preferred_element_type=F32)[:8]
    t = lax.rem(lax.broadcasted_iota(jnp.int32, start.shape, 1), steps).astype(F32)
    spot = jnp.where(t < length, start + t, -1.0)
    for d in range(owners):
        where_ref[d : d + 1, :] = spot[:1, d * rows : (d + 1) * rows]


def call_plan(steps, owners, side):
    out = jax.ShapeDtypeStruct((owners, side.shape[0]), F32)
    return pl.pallas_call(
        functools.partial(plan, steps),
        grid=(1,),
        in_specs=[whole(side.shape)],
        out_specs=whole(out.shape),
        out_shape=out,
        compiler_params=params("arbitrary"),
        name="plan",
    )(side)


def load(layer, after_ref, state_hbm, out_ref, sem):
    copy = pltpu.make_async_copy(state_hbm.at[layer], out_ref, sem)
    copy.start()
    copy.wait()


def call_load(layer, after, state):
    return pl.pallas_call(
        functools.partial(load, layer),
        grid=(1,),
        in_specs=[whole(after.shape), pl.BlockSpec(memory_space=pltpu.MemorySpace.HBM)],
        out_specs=pl.BlockSpec(memory_space=pltpu.MemorySpace.VMEM),
        out_shape=pltpu.VMEM(state.shape[1:], F32),
        scratch_shapes=[pltpu.SemaphoreType.DMA],
        compiler_params=params("arbitrary"),
        name="load_state",
    )(after, in_hbm(state))


def update(steps, wk_ref, v_ref, end_ref, state_ref, *refs):
    out_ref = refs[-1]
    for s in range(state_ref.shape[0]):
        keys = wk_ref[s * steps : (s + 1) * steps, :]
        values = v_ref[s * steps : (s + 1) * steps, :]
        fresh = lax.dot_general(keys, values, (((0,), (0,)), ((), ())), preferred_element_type=F32)
        end = end_ref[s]
        keep = jnp.transpose(jnp.broadcast_to(end, (end.shape[1], end.shape[1])))[:, :1]
        out_ref[0, s] = keep * state_ref[s] + fresh


def call_update(layer, layers, steps, wk, v, end, state, previous):
    seqs, key_dim, value_dim = state.shape
    step_seqs = 4
    block = pl.BlockSpec((1, step_seqs, key_dim, value_dim), lambda i: (layer, i, 0, 0))
    operands = [wk, v, end, state]
    in_specs = [
        pl.BlockSpec((step_seqs * steps, key_dim), lambda i: (i, 0)),
        pl.BlockSpec((step_seqs * steps, value_dim), lambda i: (i, 0)),
        pl.BlockSpec((step_seqs, 1, key_dim), lambda i: (i, 0, 0)),
        pl.BlockSpec((step_seqs, key_dim, value_dim), lambda i: (i, 0, 0)),
    ]
    alias = {}
    if previous is not None:
        operands.append(previous)
        in_specs.append(pl.BlockSpec(memory_space=pl.ANY))
        alias = {4: 0}
    return pl.pallas_call(
        functools.partial(update, steps),
        grid=(seqs // step_seqs,),
        in_specs=in_specs,
        out_specs=block,
        out_shape=jax.ShapeDtypeStruct((layers, *state.shape), F32),
        input_output_aliases=alias,
        compiler_params=params("arbitrary"),
        name="update_state",
    )(*operands)


def target_ids(meta, shape, span):
    row = lax.broadcasted_iota(jnp.int32, shape, 0)
    block = lax.rem(meta[8] + row // (ROUNDS * span), ROUNDS) + ROUNDS * lax.rem(row // span, ROUNDS)
    return (block * span + lax.rem(row, span)).astype(F32)


def close(tp, meta, where_ref, *refs):
    *g_refs, c_ref, own, plus, minus, far = refs
    rows = where_ref.shape[1]
    n = own.shape[0]
    count = n * ROUNDS
    span = count // tp
    ids = target_ids(meta, (count, rows), span)
    gathered = jnp.zeros((count, c_ref.shape[1]), F32)
    i = 0
    for g in g_refs:
        for b in range(g.shape[0]):
            chosen = (ids == where_ref[pl.ds(meta[16 + i], 1), :]).astype(F32).astype(BF)
            gathered = gathered + dot(chosen, g[b])
            i += 1
    y = dot(gathered.astype(BF), c_ref[0])
    own[...] = y[:n]
    plus[...] = y[n : 2 * n].astype(BF)
    far[...] = y[2 * n : 3 * n].astype(BF)
    minus[...] = y[3 * n :].astype(BF)


def call_close(tp, meta, where, gs, closing, live_rows):
    width = closing.shape[2]
    n = live_rows // ROUNDS
    out_shape = [
        jax.ShapeDtypeStruct((n, width), F32),
        jax.ShapeDtypeStruct((n, width), BF),
        jax.ShapeDtypeStruct((n, width), BF),
        jax.ShapeDtypeStruct((n, width), BF),
    ]
    return pl.pallas_call(
        functools.partial(close, tp),
        grid_spec=pltpu.PrefetchScalarGridSpec(
            num_scalar_prefetch=1,
            grid=(1,),
            in_specs=[
                whole(where.shape),
                *(whole(g.shape) for g in gs),
                pl.BlockSpec((1, *closing.shape[1:]), lambda i, meta: (meta[10], 0, 0)),
            ],
            out_specs=[whole(o.shape) for o in out_shape],
        ),
        out_shape=out_shape,
        compiler_params=params("arbitrary"),
        name="close",
    )(meta, where, *gs, closing)


def own_rows(span, meta, where_ref, x_ref, out_ref):
    rows = where_ref.shape[1]
    ids = target_ids(meta, (out_ref.shape[0], rows), span)
    total = jnp.zeros(out_ref.shape, F32)
    for d in range(where_ref.shape[0]):
        chosen = (ids == where_ref[d : d + 1, :]).astype(F32).astype(BF)
        total = total + dot(chosen, x_ref[d * rows : (d + 1) * rows, :])
    out_ref[...] = total.astype(BF)


def call_own_rows(tp, meta, where, x, live_rows):
    out = jax.ShapeDtypeStruct((live_rows // ROUNDS, x.shape[1]), BF)
    return pl.pallas_call(
        functools.partial(own_rows, live_rows // tp),
        grid_spec=pltpu.PrefetchScalarGridSpec(
            num_scalar_prefetch=1,
            grid=(1,),
            in_specs=[whole(where.shape), whole(x.shape)],
            out_specs=whole(out.shape),
        ),
        out_shape=out,
        compiler_params=params("arbitrary"),
        name="own_rows",
    )(meta, where, x)


def to_chip(x, step):
    n = lax.axis_size("dp")
    return lax.ppermute(x, "dp", [(d, (d + 2 * step) % n) for d in range(n)])


def to_core(x):
    n = lax.axis_size("dp")
    return lax.ppermute(x, "dp", [(d, d ^ 1) for d in range(n)])


def along(x, step):
    n = lax.axis_size("tp")
    return lax.ppermute(x, "tp", [(i, (i + step) % n) for i in range(n)])


def across(x, flip):
    n = lax.axis_size("tp")
    return lax.ppermute(x, "tp", [(i, ROUNDS * ((i // ROUNDS) ^ flip) + i % ROUNDS) for i in range(n)])


def dp_sum(send, mine, fetch):
    core = to_core(send)

    def both(j, h):
        return mine[j, h].astype(F32) + core[j, h].astype(F32)

    far_a = to_chip(both(2, 0).astype(BF), 1)
    far_b = to_chip(both(2, 1).astype(BF), -1)
    up = jnp.stack([both(1, 0) + far_a.astype(F32), both(1, 1)]).astype(BF)
    down = jnp.stack([both(3, 0), both(3, 1) + far_b.astype(F32)]).astype(BF)
    state = fetch(far_b[:8, :128])
    up, down = to_chip(up, 1), to_chip(down, -1)
    up, state = lax.optimization_barrier((up, state))
    return (mine, core, up, down), state


def dp_gather(g):
    n = lax.axis_size("dp")
    far = to_chip(g, -2)
    near = jnp.stack([g, to_chip(g, -1), far, to_chip(g, 1)])
    pairs = [[d, d + 1] for d in range(0, n, 2)]
    return lax.all_gather(near, "dp", axis_index_groups=pairs, tiled=True)


def tp_sum(parts, x_own, update):
    own, plus, minus, far = parts
    total = own + along(far, 2).astype(F32)
    total = total + along(plus, 1).astype(F32) + along(minus, -1).astype(F32)
    total = total.astype(BF)
    half = total.shape[1] // 2
    left, right = total[:, :half], total[:, half:]

    def add(a, b):
        return (a.astype(F32) + b.astype(F32)).astype(BF)

    x_own, total, state = update(x_own, total)
    got_left, got_right = across(left, 1), across(right, 3)
    got_left, x_own = lax.optimization_barrier((got_left, x_own))
    left, right = add(left, got_left), add(right, got_right)
    got_left, got_right = across(left, 3), across(right, 1)
    mixed = jnp.concatenate(
        [left.astype(F32) + got_left.astype(F32), right.astype(F32) + got_right.astype(F32)], axis=1
    )
    return (x_own.astype(F32) + mixed).astype(BF), state


def tp_gather(own):
    far = along(own, -2)
    plus = along(own, -1)
    minus = along(own, 1)
    return own, plus, minus, far


def shards(
    skip_path_activations,
    novel_lengths_per_sequence,
    input_normalizer_scales,
    question_projector,
    lookup_projector,
    payload_projector,
    emitted_valve_projector,
    keeping_valve_projector,
    keeping_valve_shift,
    additional_dwindle_exponent,
    headwise_normalizer_scales,
    closing_projector,
    earlier_recurrence_grid,
):
    streams, steps, width = skip_path_activations.shape
    dp, tp = lax.axis_size("dp"), lax.axis_size("tp")
    chips = dp // 2
    full_width = width * dp
    live_rows = streams * steps // 2
    x = skip_path_activations.reshape(streams * steps, width)
    lens = novel_lengths_per_sequence
    gain = input_normalizer_scales
    weights = (
        question_projector,
        lookup_projector,
        payload_projector,
        emitted_valve_projector,
        keeping_valve_projector,
    )
    layers, seqs, heads, key_dim, value_dim = earlier_recurrence_grid.shape
    state = earlier_recurrence_grid.reshape(layers, seqs * heads, key_dim, value_dim)
    extra = additional_dwindle_exponent.reshape(seqs * steps, 1)

    me = lax.axis_index("dp")
    slot = lax.iota(jnp.int32, 32)
    side_core = (slot // chips) % 2
    owner = 2 * ((me // 2 + slot) % chips) + jnp.where(slot < 16, (me % 2) ^ side_core, side_core)
    meta = jnp.where(slot == 8, lax.axis_index("tp"), jnp.where(slot == 9, me, owner)).astype(jnp.int32)
    metas = [jnp.where(slot == 10, layer, meta) for layer in range(layers)]
    other = meta ^ (slot < 2 * chips)

    new_state = None
    where = x_own = pieces = None
    for layer in range(layers):
        if layer == 0:
            run = lambda order: call_project_first(layer, order, in_hbm(lens), x, gain, weights, chips)
        else:
            run = lambda order: call_project_next(layer, order, where, pieces, gain, weights, chips)
        send, mine = [run(order) for order in (other, metas[layer])]
        parts, held = dp_sum(send, mine, lambda after: call_load(layer, after, state))
        g, wk, v, end, side = call_recur(
            metas[layer], full_width, lens, parts, keeping_valve_shift, extra,
            headwise_normalizer_scales, held, steps,
        )
        if layer == 0:
            where = call_plan(steps, dp, side)
            x_own = call_own_rows(tp, meta, where, x, live_rows)
        sums = call_close(tp, metas[layer], where, [dp_gather(g)], closing_projector, live_rows)

        def update(own, total):
            total, keys = lax.optimization_barrier((total, wk))
            fresh = call_update(layer, layers, steps, keys, v, end, held, new_state)
            own, fresh = lax.optimization_barrier((own, fresh))
            return own, total, fresh

        x_own, new_state = tp_sum(sums, x_own, update)
        pieces = tp_gather(x_own)
    stream = call_finish(meta, where, pieces, x)
    return (
        stream.reshape(streams, steps, width),
        new_state.reshape(earlier_recurrence_grid.shape),
    )


def solution(mesh):
    in_specs = (
        P("grp", None, "dp"),
        P(("grp", "dp")),
        P(None, "dp"),
        P(None, "dp", "tp"),
        P(None, "dp", "tp"),
        P(None, "dp", "tp"),
        P(None, "dp", "tp"),
        P(None, "dp", "tp"),
        P(None, "tp"),
        P(("grp", "dp"), None, "tp"),
        P(),
        P(None, "tp", "dp"),
        P(None, ("grp", "dp"), "tp", None, None),
    )
    out_specs = (P("grp", None, "dp"), P(None, ("grp", "dp"), "tp", None, None))
    return jax.shard_map(shards, mesh=mesh, in_specs=in_specs, out_specs=out_specs, check_vma=False)
```

```python
import functools

import jax
import jax.numpy as jnp
from jax import lax
from jax.experimental import pallas as pl
from jax.experimental.pallas import tpu as pltpu
from jax.sharding import PartitionSpec as P


EPS = 1e-06
TAU = 16.0
BF = jnp.bfloat16
F32 = jnp.float32
VMEM_LIMIT = 8 * 1024 * 1024
ROUNDS = 4
SIDE = 128


def dot(a, b):
    return jnp.dot(a, b, preferred_element_type=F32)


def params(*semantics):
    return pltpu.CompilerParams(vmem_limit_bytes=VMEM_LIMIT, dimension_semantics=semantics or None)


def row_of(ref, layer):
    row = ref[0:1, :]
    for i in range(1, ref.shape[0]):
        row = jnp.where(layer == i, ref[i : i + 1, :], row)
    return row


def in_hbm(x):
    return pltpu.with_memory_space_constraint(x, pltpu.MemorySpace.HBM)


def whole(shape):
    return pl.BlockSpec(shape, lambda *_: (0,) * len(shape))


def project(layer, x, gain_ref, w_refs, out_ref, lens_col):
    blocks, _, rows, _ = out_ref.shape
    xf = x.astype(F32)
    gain = row_of(gain_ref, layer).astype(F32)
    scaled = jnp.clip(xf * gain, -1e30, 1e30).astype(BF)

    def put(half, at, value):
        for j in range(blocks):
            out_ref[j, half, :, at : at + value.shape[1]] = value[j * rows : (j + 1) * rows].astype(BF)

    ends = []
    for half, group in enumerate((w_refs[:3], w_refs[3:])):
        at = 0
        for w in group:
            put(half, at, dot(scaled, w[0]))
            at += w.shape[-1]
        ends.append(at)
    squares = jnp.sum(xf * xf, axis=1, keepdims=True)
    high = squares.astype(BF).astype(F32)
    low = jnp.where(jnp.abs(high) < 3.0e38, squares - high, 0.0)
    lane = lax.broadcasted_iota(jnp.int32, (x.shape[0], SIDE), 1)
    side = jnp.where(lane == 0, high, jnp.where(lane == 1, low, 0.0))
    if lens_col is not None:
        side = jnp.where(lane == 2, lens_col, side)
    put(1, ends[1], side)


def project_first(layer, local_seqs, meta, lens, x0, x1, gain_ref, wq, wk, wv, wr, wf, out_ref):
    x = jnp.concatenate([x0[...], x1[...]], axis=0)
    rows = x0.shape[0]
    row = lax.broadcasted_iota(jnp.int32, (rows, SIDE), 0) - meta[9] * local_seqs
    lens_col = jnp.zeros((rows, SIDE), F32)
    for s in range(local_seqs):
        lens_col = jnp.where(row == s, lens[s].astype(F32), lens_col)
    lens_col = jnp.concatenate([lens_col] * 2, axis=0)
    project(layer, x, gain_ref, (wq, wk, wv, wr, wf), out_ref, lens_col)


def piece_ids(meta, shape, offset):
    span = shape[1] // ROUNDS
    lane = lax.broadcasted_iota(jnp.int32, shape, 1)
    block = lax.rem(meta[8] + offset + ROUNDS, ROUNDS) + ROUNDS * (lane // span)
    return (block * span + lax.rem(lane, span)).astype(F32)


def expand(meta, where_rows, pieces):
    own, plus, minus, far = pieces
    rows = where_rows[0].shape[1]
    place = jnp.concatenate(
        [jnp.transpose(jnp.broadcast_to(r, (rows, rows)))[:, :1] for r in where_rows], axis=0
    )
    at = jnp.broadcast_to(place, (place.shape[0], own.shape[0]))

    def chosen(offset):
        return (at == piece_ids(meta, at.shape, offset)).astype(F32).astype(BF)

    x = dot(chosen(0), own[...]) + dot(chosen(1), plus[...]) + dot(chosen(-1), minus[...])
    return x + dot(chosen(2), far[...]), place


def project_next(layer, meta, where_ref, *refs):
    *pieces, gain_ref, wq, wk, wv, wr, wf, out_ref = refs
    first = 2 * pl.program_id(0)
    rows = [where_ref[pl.ds(meta[first + j], 1), :] for j in range(2)]
    x, _ = expand(meta, rows, pieces)
    project(layer, x, gain_ref, (wq, wk, wv, wr, wf), out_ref, None)


def finish(blocks, meta, where_ref, *refs):
    *pieces, x_ref, out_ref = refs
    first = pl.program_id(0) * blocks
    rows = [where_ref[pl.ds(first + j, 1), :] for j in range(blocks)]
    live, place = expand(meta, rows, pieces)
    out_ref[...] = jnp.where(place < 0, x_ref[...].astype(F32), live).astype(BF)


def weight_spec(layer, w):
    return pl.BlockSpec((1, w.shape[1], w.shape[2]), lambda *_: (layer, 0, 0))


def projected(weights, rows, blocks):
    cols = sum(w.shape[2] for w in weights[:3])
    assert cols == sum(w.shape[2] for w in weights[3:]) + SIDE
    return jax.ShapeDtypeStruct((blocks, 2, rows, cols), BF)


def call_project_first(layer, meta, lens, x, gain, weights, blocks):
    rows, width = x.shape[0] // (2 * blocks), x.shape[1]
    out = projected(weights, rows, blocks)

    def block_of(j):
        return pl.BlockSpec((rows, width), lambda i, meta, lens: (meta[2 * i + j], 0))

    return pl.pallas_call(
        functools.partial(project_first, layer, lens.shape[0]),
        grid_spec=pltpu.PrefetchScalarGridSpec(
            num_scalar_prefetch=2,
            grid=(blocks // 2,),
            in_specs=[
                *(block_of(j) for j in range(2)),
                whole(gain.shape),
                *(weight_spec(layer, w) for w in weights),
            ],
            out_specs=pl.BlockSpec((2, *out.shape[1:]), lambda i, *_: (i, 0, 0, 0)),
        ),
        out_shape=out,
        compiler_params=params("arbitrary"),
        name="project_first",
    )(meta, lens, *([in_hbm(x)] * 2), in_hbm(gain), *(in_hbm(w) for w in weights))


def piece_specs(pieces):
    return [whole(p.shape) for p in pieces]


def call_project_next(layer, meta, where, pieces, gain, weights, blocks):
    out = projected(weights, where.shape[1], blocks)
    return pl.pallas_call(
        functools.partial(project_next, layer),
        grid_spec=pltpu.PrefetchScalarGridSpec(
            num_scalar_prefetch=1,
            grid=(blocks // 2,),
            in_specs=[
                whole(where.shape),
                *piece_specs(pieces),
                whole(gain.shape),
                *(weight_spec(layer, w) for w in weights),
            ],
            out_specs=pl.BlockSpec((2, *out.shape[1:]), lambda i, *_: (i, 0, 0, 0)),
        ),
        out_shape=out,
        compiler_params=params("arbitrary"),
        name="project_next",
    )(meta, where, *pieces, gain, *weights)


def call_finish(meta, where, pieces, x):
    owners, rows = where.shape
    blocks = owners // 2
    return pl.pallas_call(
        functools.partial(finish, blocks),
        grid_spec=pltpu.PrefetchScalarGridSpec(
            num_scalar_prefetch=1,
            grid=(owners // blocks,),
            in_specs=[
                whole(where.shape),
                *piece_specs(pieces),
                pl.BlockSpec((blocks * rows, x.shape[1]), lambda i, *_: (i, 0)),
            ],
            out_specs=pl.BlockSpec((blocks * rows, x.shape[1]), lambda i, *_: (i, 0)),
        ),
        out_shape=jax.ShapeDtypeStruct(x.shape, BF),
        compiler_params=params("arbitrary"),
        name="finish",
    )(meta, where, *pieces, x)


def recur(full_width, steps, meta, lens, *refs):
    layer = meta[10]
    (mine, core, up, down, shift_ref, extra_ref, hs_ref, state), rest = refs[:8], refs[8:]
    g_ref, wk_ref, v_ref, end_ref, side_ref = rest
    seqs, key_dim, value_dim = state.shape
    rows = seqs * steps
    sum_a, sum_b = [
        (mine[0, h].astype(F32) + core[0, h].astype(F32)) + (up[h].astype(F32) + down[h].astype(F32))
        for h in range(2)
    ]
    at = value_dim + key_dim
    side = sum_b[:, at : at + SIDE]
    squares = side[:, 0:1] + side[:, 1:2]
    rms = lax.rsqrt(squares / full_width + EPS)
    q = sum_a[:, :key_dim] * (rms * key_dim ** (-0.5))
    k = sum_a[:, key_dim : 2 * key_dim] * rms
    v = sum_a[:, 2 * key_dim :] * rms
    r = sum_b[:, :value_dim] * rms
    f = sum_b[:, value_dim:at] * rms

    row = lax.broadcasted_iota(jnp.int32, (rows, key_dim), 0)
    own_len = jnp.zeros((rows, key_dim), jnp.int32)
    for s in range(seqs):
        own_len = jnp.where(row // steps == s, lens[s], own_len)
    live = jnp.where(lax.rem(row, steps) < own_len, 1.0, 0.0)
    logits = f + row_of(shift_ref, layer)
    log_sig = jnp.minimum(logits, 0.0) - jnp.log(1.0 + jnp.exp(-jnp.abs(logits)))
    fade = (log_sig / TAU + extra_ref[...]) * live
    k = k * live

    def by_seq(x):
        return x.reshape(seqs, steps, x.shape[1])

    q3, k3, v3, fade3 = by_seq(q), by_seq(k), by_seq(v), by_seq(fade)
    slot = lax.broadcasted_iota(jnp.int32, (seqs, steps, key_dim), 1)
    total = jnp.zeros_like(fade3)
    for j in range(steps):
        total = total + jnp.where(slot >= j, fade3[:, j : j + 1, :], 0.0)
    out = jnp.zeros_like(v3)
    for j in range(steps):
        apart = jnp.where(slot >= j, total - total[:, j : j + 1, :], -1e30)
        score = jnp.sum(q3 * k3[:, j : j + 1, :] * jnp.exp(apart), axis=-1, keepdims=True)
        out = out + score * v3[:, j : j + 1, :]
    last = total[:, steps - 1 : steps, :]
    wk_ref[...] = (k3 * jnp.exp(last - total)).reshape(rows, key_dim).astype(BF)
    v_ref[...] = v.astype(BF)
    end_ref[...] = jnp.exp(last)
    side_ref[...] = side
    weighted = (q3 * jnp.exp(total)).reshape(rows, key_dim).astype(BF)
    carried = [
        dot(weighted[s * steps : (s + 1) * steps], state[s].astype(BF)) for s in range(seqs)
    ]
    out = out.reshape(rows, value_dim) + jnp.concatenate(carried, axis=0)
    scale = lax.rsqrt(jnp.mean(out * out, axis=-1, keepdims=True) + EPS)
    silu = r / (1.0 + jnp.exp(-r))
    g_ref[...] = (out * scale * row_of(hs_ref, layer).astype(F32) * silu * live[:, :1]).astype(BF)


def call_recur(meta, full_width, lens, parts, shift, extra, head_scale, state, steps):
    seqs, key_dim, value_dim = state.shape
    rows = seqs * steps
    mine, _, up, down = parts
    first = pl.BlockSpec((1, *mine.shape[1:]), lambda *_: (0, 0, 0, 0))
    out_shape = [
        jax.ShapeDtypeStruct((rows, value_dim), BF),
        jax.ShapeDtypeStruct((rows, key_dim), BF),
        jax.ShapeDtypeStruct((rows, value_dim), BF),
        jax.ShapeDtypeStruct((seqs, 1, key_dim), F32),
        jax.ShapeDtypeStruct((rows, SIDE), F32),
    ]
    return pl.pallas_call(
        functools.partial(recur, full_width, steps),
        grid_spec=pltpu.PrefetchScalarGridSpec(
            num_scalar_prefetch=2,
            grid=(1,),
            in_specs=[
                first,
                first,
                whole(up.shape),
                whole(down.shape),
                whole(shift.shape),
                whole((rows, 1)),
                whole(head_scale.shape),
                whole(state.shape),
            ],
            out_specs=[whole(o.shape) for o in out_shape],
        ),
        out_shape=out_shape,
        compiler_params=params("arbitrary"),
        name="recur",
    )(meta, lens, *parts, shift, extra, head_scale, state)


def plan(steps, side_ref, where_ref):
    side = side_ref[...]
    rows = where_ref.shape[1]
    owners = where_ref.shape[0]
    n = side.shape[0]
    lens_all = jnp.broadcast_to(side[:, 2:3], side.shape).astype(BF)
    seq_of = lax.broadcasted_iota(jnp.int32, (n, owners * rows), 1) // steps
    seq = lax.broadcasted_iota(jnp.int32, (n, owners * rows), 0)
    before = (seq < seq_of).astype(F32).astype(BF)
    same = (seq == seq_of).astype(F32).astype(BF)
    over = (((0,), (0,)), ((), ()))
    start = lax.dot_general(lens_all, before, over, preferred_element_type=F32)[:8]
    length = lax.dot_general(lens_all, same, over, preferred_element_type=F32)[:8]
    t = lax.rem(lax.broadcasted_iota(jnp.int32, start.shape, 1), steps).astype(F32)
    spot = jnp.where(t < length, start + t, -1.0)
    for d in range(owners):
        where_ref[d : d + 1, :] = spot[:1, d * rows : (d + 1) * rows]


def call_plan(steps, owners, side):
    out = jax.ShapeDtypeStruct((owners, side.shape[0]), F32)
    return pl.pallas_call(
        functools.partial(plan, steps),
        grid=(1,),
        in_specs=[whole(side.shape)],
        out_specs=whole(out.shape),
        out_shape=out,
        compiler_params=params("arbitrary"),
        name="plan",
    )(side)


def load(layer, after_ref, state_hbm, out_ref, sem):
    copy = pltpu.make_async_copy(state_hbm.at[layer], out_ref, sem)
    copy.start()
    copy.wait()


def call_load(layer, after, state):
    return pl.pallas_call(
        functools.partial(load, layer),
        grid=(1,),
        in_specs=[whole(after.shape), pl.BlockSpec(memory_space=pltpu.MemorySpace.HBM)],
        out_specs=pl.BlockSpec(memory_space=pltpu.MemorySpace.VMEM),
        out_shape=pltpu.VMEM(state.shape[1:], F32),
        scratch_shapes=[pltpu.SemaphoreType.DMA],
        compiler_params=params("arbitrary"),
        name="load_state",
    )(after, in_hbm(state))


def update(steps, wk_ref, v_ref, end_ref, state_ref, *refs):
    out_ref = refs[-1]
    for s in range(state_ref.shape[0]):
        keys = wk_ref[s * steps : (s + 1) * steps, :]
        values = v_ref[s * steps : (s + 1) * steps, :]
        fresh = lax.dot_general(keys, values, (((0,), (0,)), ((), ())), preferred_element_type=F32)
        end = end_ref[s]
        keep = jnp.transpose(jnp.broadcast_to(end, (end.shape[1], end.shape[1])))[:, :1]
        out_ref[0, s] = keep * state_ref[s] + fresh


def call_update(layer, layers, steps, wk, v, end, state, previous):
    seqs, key_dim, value_dim = state.shape
    step_seqs = 4
    block = pl.BlockSpec((1, step_seqs, key_dim, value_dim), lambda i: (layer, i, 0, 0))
    operands = [wk, v, end, state]
    in_specs = [
        pl.BlockSpec((step_seqs * steps, key_dim), lambda i: (i, 0)),
        pl.BlockSpec((step_seqs * steps, value_dim), lambda i: (i, 0)),
        pl.BlockSpec((step_seqs, 1, key_dim), lambda i: (i, 0, 0)),
        pl.BlockSpec((step_seqs, key_dim, value_dim), lambda i: (i, 0, 0)),
    ]
    alias = {}
    if previous is not None:
        operands.append(previous)
        in_specs.append(pl.BlockSpec(memory_space=pl.ANY))
        alias = {4: 0}
    return pl.pallas_call(
        functools.partial(update, steps),
        grid=(seqs // step_seqs,),
        in_specs=in_specs,
        out_specs=block,
        out_shape=jax.ShapeDtypeStruct((layers, *state.shape), F32),
        input_output_aliases=alias,
        compiler_params=params("arbitrary"),
        name="update_state",
    )(*operands)


def target_ids(meta, shape, span):
    row = lax.broadcasted_iota(jnp.int32, shape, 0)
    block = lax.rem(meta[8] + row // (ROUNDS * span), ROUNDS) + ROUNDS * lax.rem(row // span, ROUNDS)
    return (block * span + lax.rem(row, span)).astype(F32)


def close(tp, meta, where_ref, *refs):
    *g_refs, c_ref, own, plus, minus, far = refs
    rows = where_ref.shape[1]
    n = own.shape[0]
    count = n * ROUNDS
    span = count // tp
    ids = target_ids(meta, (count, rows), span)
    gathered = jnp.zeros((count, c_ref.shape[1]), F32)
    i = 0
    for g in g_refs:
        for b in range(g.shape[0]):
            chosen = (ids == where_ref[pl.ds(meta[16 + i], 1), :]).astype(F32).astype(BF)
            gathered = gathered + dot(chosen, g[b])
            i += 1
    y = dot(gathered.astype(BF), c_ref[0])
    own[...] = y[:n]
    plus[...] = y[n : 2 * n].astype(BF)
    far[...] = y[2 * n : 3 * n].astype(BF)
    minus[...] = y[3 * n :].astype(BF)


def call_close(tp, meta, where, gs, closing, live_rows):
    width = closing.shape[2]
    n = live_rows // ROUNDS
    out_shape = [
        jax.ShapeDtypeStruct((n, width), F32),
        jax.ShapeDtypeStruct((n, width), BF),
        jax.ShapeDtypeStruct((n, width), BF),
        jax.ShapeDtypeStruct((n, width), BF),
    ]
    return pl.pallas_call(
        functools.partial(close, tp),
        grid_spec=pltpu.PrefetchScalarGridSpec(
            num_scalar_prefetch=1,
            grid=(1,),
            in_specs=[
                whole(where.shape),
                *(whole(g.shape) for g in gs),
                pl.BlockSpec((1, *closing.shape[1:]), lambda i, meta: (meta[10], 0, 0)),
            ],
            out_specs=[whole(o.shape) for o in out_shape],
        ),
        out_shape=out_shape,
        compiler_params=params("arbitrary"),
        name="close",
    )(meta, where, *gs, closing)


def own_rows(span, meta, where_ref, x_ref, out_ref):
    rows = where_ref.shape[1]
    ids = target_ids(meta, (out_ref.shape[0], rows), span)
    total = jnp.zeros(out_ref.shape, F32)
    for d in range(where_ref.shape[0]):
        chosen = (ids == where_ref[d : d + 1, :]).astype(F32).astype(BF)
        total = total + dot(chosen, x_ref[d * rows : (d + 1) * rows, :])
    out_ref[...] = total.astype(BF)


def call_own_rows(tp, meta, where, x, live_rows):
    out = jax.ShapeDtypeStruct((live_rows // ROUNDS, x.shape[1]), BF)
    return pl.pallas_call(
        functools.partial(own_rows, live_rows // tp),
        grid_spec=pltpu.PrefetchScalarGridSpec(
            num_scalar_prefetch=1,
            grid=(1,),
            in_specs=[whole(where.shape), whole(x.shape)],
            out_specs=whole(out.shape),
        ),
        out_shape=out,
        compiler_params=params("arbitrary"),
        name="own_rows",
    )(meta, where, x)


def to_chip(x, step):
    n = lax.axis_size("dp")
    return lax.ppermute(x, "dp", [(d, (d + 2 * step) % n) for d in range(n)])


def to_core(x):
    n = lax.axis_size("dp")
    return lax.ppermute(x, "dp", [(d, d ^ 1) for d in range(n)])


def along(x, step):
    n = lax.axis_size("tp")
    return lax.ppermute(x, "tp", [(i, (i + step) % n) for i in range(n)])


def across(x, flip):
    n = lax.axis_size("tp")
    return lax.ppermute(x, "tp", [(i, ROUNDS * ((i // ROUNDS) ^ flip) + i % ROUNDS) for i in range(n)])


def dp_sum(send, mine, fetch):
    core = to_core(send)

    def both(j, h):
        return mine[j, h].astype(F32) + core[j, h].astype(F32)

    far_a = to_chip(both(2, 0).astype(BF), 1)
    far_b = to_chip(both(2, 1).astype(BF), -1)
    up = jnp.stack([both(1, 0) + far_a.astype(F32), both(1, 1)]).astype(BF)
    down = jnp.stack([both(3, 0), both(3, 1) + far_b.astype(F32)]).astype(BF)
    state = fetch(far_b[:8, :128])
    up, down = to_chip(up, 1), to_chip(down, -1)
    up, state = lax.optimization_barrier((up, state))
    return (mine, core, up, down), state


def dp_gather(g):
    n = lax.axis_size("dp")
    far = to_chip(g, -2)
    near = jnp.stack([g, to_chip(g, -1), far, to_chip(g, 1)])
    pairs = [[d, d + 1] for d in range(0, n, 2)]
    return lax.all_gather(near, "dp", axis_index_groups=pairs, tiled=True)


def tp_sum(parts, x_own, update):
    own, plus, minus, far = parts
    total = own + along(far, 2).astype(F32)
    total = total + along(plus, 1).astype(F32) + along(minus, -1).astype(F32)
    total = total.astype(BF)
    half = total.shape[1] // 2
    left, right = total[:, :half], total[:, half:]

    def add(a, b):
        return (a.astype(F32) + b.astype(F32)).astype(BF)

    x_own, total, state = update(x_own, total)
    got_left, got_right = across(left, 1), across(right, 3)
    got_left, x_own = lax.optimization_barrier((got_left, x_own))
    left, right = add(left, got_left), add(right, got_right)
    got_left, got_right = across(left, 3), across(right, 1)
    mixed = jnp.concatenate(
        [left.astype(F32) + got_left.astype(F32), right.astype(F32) + got_right.astype(F32)], axis=1
    )
    return (x_own.astype(F32) + mixed).astype(BF), state


def tp_gather(own):
    far = along(own, -2)
    plus = along(own, -1)
    minus = along(own, 1)
    return own, plus, minus, far


def shards(
    skip_path_activations,
    novel_lengths_per_sequence,
    input_normalizer_scales,
    question_projector,
    lookup_projector,
    payload_projector,
    emitted_valve_projector,
    keeping_valve_projector,
    keeping_valve_shift,
    additional_dwindle_exponent,
    headwise_normalizer_scales,
    closing_projector,
    earlier_recurrence_grid,
):
    streams, steps, width = skip_path_activations.shape
    dp, tp = lax.axis_size("dp"), lax.axis_size("tp")
    chips = dp // 2
    full_width = width * dp
    live_rows = streams * steps // 2
    x = skip_path_activations.reshape(streams * steps, width)
    lens = novel_lengths_per_sequence
    gain = input_normalizer_scales
    weights = (
        question_projector,
        lookup_projector,
        payload_projector,
        emitted_valve_projector,
        keeping_valve_projector,
    )
    layers, seqs, heads, key_dim, value_dim = earlier_recurrence_grid.shape
    state = earlier_recurrence_grid.reshape(layers, seqs * heads, key_dim, value_dim)
    extra = additional_dwindle_exponent.reshape(seqs * steps, 1)

    me = lax.axis_index("dp")
    slot = lax.iota(jnp.int32, 32)
    side_core = (slot // chips) % 2
    owner = 2 * ((me // 2 + slot) % chips) + jnp.where(slot < 16, (me % 2) ^ side_core, side_core)
    meta = jnp.where(slot == 8, lax.axis_index("tp"), jnp.where(slot == 9, me, owner)).astype(jnp.int32)
    metas = [jnp.where(slot == 10, layer, meta) for layer in range(layers)]
    other = meta ^ (slot < 2 * chips)

    new_state = None
    where = x_own = pieces = None
    for layer in range(layers):
        if layer == 0:
            run = lambda order: call_project_first(layer, order, in_hbm(lens), x, gain, weights, chips)
        else:
            run = lambda order: call_project_next(layer, order, where, pieces, gain, weights, chips)
        send, mine = [run(order) for order in (other, metas[layer])]
        parts, held = dp_sum(send, mine, lambda after: call_load(layer, after, state))
        g, wk, v, end, side = call_recur(
            metas[layer], full_width, lens, parts, keeping_valve_shift, extra,
            headwise_normalizer_scales, held, steps,
        )
        if layer == 0:
            where = call_plan(steps, dp, side)
            x_own = call_own_rows(tp, meta, where, x, live_rows)
        sums = call_close(tp, metas[layer], where, [dp_gather(g)], closing_projector, live_rows)

        def update(own, total):
            total, keys = lax.optimization_barrier((total, wk))
            fresh = call_update(layer, layers, steps, keys, v, end, held, new_state)
            own, fresh = lax.optimization_barrier((own, fresh))
            return own, total, fresh

        x_own, new_state = tp_sum(sums, x_own, update)
        pieces = tp_gather(x_own)
    stream = call_finish(meta, where, pieces, x)
    return (
        stream.reshape(streams, steps, width),
        new_state.reshape(earlier_recurrence_grid.shape),
    )


def solution(mesh):
    in_specs = (
        P("grp", None, "dp"),
        P(("grp", "dp")),
        P(None, "dp"),
        P(None, "dp", "tp"),
        P(None, "dp", "tp"),
        P(None, "dp", "tp"),
        P(None, "dp", "tp"),
        P(None, "dp", "tp"),
        P(None, "tp"),
        P(("grp", "dp"), None, "tp"),
        P(),
        P(None, "tp", "dp"),
        P(None, ("grp", "dp"), "tp", None, None),
    )
    out_specs = (P("grp", None, "dp"), P(None, ("grp", "dp"), "tp", None, None))
    return jax.shard_map(shards, mesh=mesh, in_specs=in_specs, out_specs=out_specs, check_vma=False)
```

```python
import functools

import jax
import jax.numpy as jnp
from jax import lax
from jax.experimental import pallas as pl
from jax.experimental.pallas import tpu as pltpu
from jax.sharding import PartitionSpec as P


EPS = 1e-06
TAU = 16.0
BF = jnp.bfloat16
F32 = jnp.float32
VMEM_LIMIT = 8 * 1024 * 1024
ROUNDS = 4
SIDE = 128


def dot(a, b):
    return jnp.dot(a, b, preferred_element_type=F32)


def params(*semantics):
    return pltpu.CompilerParams(vmem_limit_bytes=VMEM_LIMIT, dimension_semantics=semantics or None)


def row_of(ref, layer):
    row = ref[0:1, :]
    for i in range(1, ref.shape[0]):
        row = jnp.where(layer == i, ref[i : i + 1, :], row)
    return row


def in_hbm(x):
    return pltpu.with_memory_space_constraint(x, pltpu.MemorySpace.HBM)


def whole(shape):
    return pl.BlockSpec(shape, lambda *_: (0,) * len(shape))


def project(layer, x, gain_ref, w_refs, out_ref, lens_col):
    blocks, _, rows, _ = out_ref.shape
    xf = x.astype(F32)
    gain = row_of(gain_ref, layer).astype(F32)
    scaled = jnp.clip(xf * gain, -1e30, 1e30).astype(BF)

    def put(half, at, value):
        for j in range(blocks):
            out_ref[j, half, :, at : at + value.shape[1]] = value[j * rows : (j + 1) * rows].astype(BF)

    ends = []
    for half, group in enumerate((w_refs[:3], w_refs[3:])):
        at = 0
        for w in group:
            put(half, at, dot(scaled, w[0]))
            at += w.shape[-1]
        ends.append(at)
    squares = jnp.sum(xf * xf, axis=1, keepdims=True)
    high = squares.astype(BF).astype(F32)
    low = jnp.where(jnp.abs(high) < 3.0e38, squares - high, 0.0)
    lane = lax.broadcasted_iota(jnp.int32, (x.shape[0], SIDE), 1)
    side = jnp.where(lane == 0, high, jnp.where(lane == 1, low, 0.0))
    if lens_col is not None:
        side = jnp.where(lane == 2, lens_col, side)
    put(1, ends[1], side)


def project_first(layer, local_seqs, meta, lens, x0, x1, gain_ref, wq, wk, wv, wr, wf, out_ref):
    x = jnp.concatenate([x0[...], x1[...]], axis=0)
    rows = x0.shape[0]
    row = lax.broadcasted_iota(jnp.int32, (rows, SIDE), 0) - meta[9] * local_seqs
    lens_col = jnp.zeros((rows, SIDE), F32)
    for s in range(local_seqs):
        lens_col = jnp.where(row == s, lens[s].astype(F32), lens_col)
    lens_col = jnp.concatenate([lens_col] * 2, axis=0)
    project(layer, x, gain_ref, (wq, wk, wv, wr, wf), out_ref, lens_col)


def piece_ids(meta, shape, offset):
    span = shape[1] // ROUNDS
    lane = lax.broadcasted_iota(jnp.int32, shape, 1)
    block = lax.rem(meta[8] + offset + ROUNDS, ROUNDS) + ROUNDS * (lane // span)
    return (block * span + lax.rem(lane, span)).astype(F32)


def expand(meta, where_rows, pieces):
    own, plus, minus, far = pieces
    rows = where_rows[0].shape[1]
    place = jnp.concatenate(
        [jnp.transpose(jnp.broadcast_to(r, (rows, rows)))[:, :1] for r in where_rows], axis=0
    )
    at = jnp.broadcast_to(place, (place.shape[0], own.shape[0]))

    def chosen(offset):
        return (at == piece_ids(meta, at.shape, offset)).astype(F32).astype(BF)

    x = dot(chosen(0), own[...]) + dot(chosen(1), plus[...]) + dot(chosen(-1), minus[...])
    return x + dot(chosen(2), far[...]), place


def project_next(layer, meta, where_ref, *refs):
    *pieces, gain_ref, wq, wk, wv, wr, wf, out_ref = refs
    first = 2 * pl.program_id(0)
    rows = [where_ref[pl.ds(meta[first + j], 1), :] for j in range(2)]
    x, _ = expand(meta, rows, pieces)
    project(layer, x, gain_ref, (wq, wk, wv, wr, wf), out_ref, None)


def finish(blocks, meta, where_ref, *refs):
    *pieces, x_ref, out_ref = refs
    first = pl.program_id(0) * blocks
    rows = [where_ref[pl.ds(first + j, 1), :] for j in range(blocks)]
    live, place = expand(meta, rows, pieces)
    out_ref[...] = jnp.where(place < 0, x_ref[...].astype(F32), live).astype(BF)


def weight_spec(layer, w):
    return pl.BlockSpec((1, w.shape[1], w.shape[2]), lambda *_: (layer, 0, 0))


def projected(weights, rows, blocks):
    cols = sum(w.shape[2] for w in weights[:3])
    assert cols == sum(w.shape[2] for w in weights[3:]) + SIDE
    return jax.ShapeDtypeStruct((blocks, 2, rows, cols), BF)


def call_project_first(layer, meta, lens, x, gain, weights, blocks):
    rows, width = x.shape[0] // (2 * blocks), x.shape[1]
    out = projected(weights, rows, blocks)

    def block_of(j):
        return pl.BlockSpec((rows, width), lambda i, meta, lens: (meta[2 * i + j], 0))

    return pl.pallas_call(
        functools.partial(project_first, layer, lens.shape[0]),
        grid_spec=pltpu.PrefetchScalarGridSpec(
            num_scalar_prefetch=2,
            grid=(blocks // 2,),
            in_specs=[
                *(block_of(j) for j in range(2)),
                whole(gain.shape),
                *(weight_spec(layer, w) for w in weights),
            ],
            out_specs=pl.BlockSpec((2, *out.shape[1:]), lambda i, *_: (i, 0, 0, 0)),
        ),
        out_shape=out,
        compiler_params=params("arbitrary"),
        name="project_first",
    )(meta, lens, *([in_hbm(x)] * 2), in_hbm(gain), *(in_hbm(w) for w in weights))


def piece_specs(pieces):
    return [whole(p.shape) for p in pieces]


def call_project_next(layer, meta, where, pieces, gain, weights, blocks):
    out = projected(weights, where.shape[1], blocks)
    return pl.pallas_call(
        functools.partial(project_next, layer),
        grid_spec=pltpu.PrefetchScalarGridSpec(
            num_scalar_prefetch=1,
            grid=(blocks // 2,),
            in_specs=[
                whole(where.shape),
                *piece_specs(pieces),
                whole(gain.shape),
                *(weight_spec(layer, w) for w in weights),
            ],
            out_specs=pl.BlockSpec((2, *out.shape[1:]), lambda i, *_: (i, 0, 0, 0)),
        ),
        out_shape=out,
        compiler_params=params("arbitrary"),
        name="project_next",
    )(meta, where, *pieces, gain, *weights)


def call_finish(meta, where, pieces, x):
    owners, rows = where.shape
    blocks = owners // 2
    return pl.pallas_call(
        functools.partial(finish, blocks),
        grid_spec=pltpu.PrefetchScalarGridSpec(
            num_scalar_prefetch=1,
            grid=(owners // blocks,),
            in_specs=[
                whole(where.shape),
                *piece_specs(pieces),
                pl.BlockSpec((blocks * rows, x.shape[1]), lambda i, *_: (i, 0)),
            ],
            out_specs=pl.BlockSpec((blocks * rows, x.shape[1]), lambda i, *_: (i, 0)),
        ),
        out_shape=jax.ShapeDtypeStruct(x.shape, BF),
        compiler_params=params("arbitrary"),
        name="finish",
    )(meta, where, *pieces, x)


def recur(full_width, steps, meta, lens, *refs):
    layer = meta[10]
    (mine, core, up, down, shift_ref, extra_ref, hs_ref, state), rest = refs[:8], refs[8:]
    g_ref, wk_ref, v_ref, end_ref, side_ref = rest
    seqs, key_dim, value_dim = state.shape
    rows = seqs * steps
    sum_a, sum_b = [
        (mine[0, h].astype(F32) + core[0, h].astype(F32)) + (up[h].astype(F32) + down[h].astype(F32))
        for h in range(2)
    ]
    at = value_dim + key_dim
    side = sum_b[:, at : at + SIDE]
    squares = side[:, 0:1] + side[:, 1:2]
    rms = lax.rsqrt(squares / full_width + EPS)
    q = sum_a[:, :key_dim] * (rms * key_dim ** (-0.5))
    k = sum_a[:, key_dim : 2 * key_dim] * rms
    v = sum_a[:, 2 * key_dim :] * rms
    r = sum_b[:, :value_dim] * rms
    f = sum_b[:, value_dim:at] * rms

    row = lax.broadcasted_iota(jnp.int32, (rows, key_dim), 0)
    own_len = jnp.zeros((rows, key_dim), jnp.int32)
    for s in range(seqs):
        own_len = jnp.where(row // steps == s, lens[s], own_len)
    live = jnp.where(lax.rem(row, steps) < own_len, 1.0, 0.0)
    logits = f + row_of(shift_ref, layer)
    log_sig = jnp.minimum(logits, 0.0) - jnp.log(1.0 + jnp.exp(-jnp.abs(logits)))
    fade = (log_sig / TAU + extra_ref[...]) * live
    k = k * live

    def by_seq(x):
        return x.reshape(seqs, steps, x.shape[1])

    q3, k3, v3, fade3 = by_seq(q), by_seq(k), by_seq(v), by_seq(fade)
    slot = lax.broadcasted_iota(jnp.int32, (seqs, steps, key_dim), 1)
    total = jnp.zeros_like(fade3)
    for j in range(steps):
        total = total + jnp.where(slot >= j, fade3[:, j : j + 1, :], 0.0)
    out = jnp.zeros_like(v3)
    for j in range(steps):
        apart = jnp.where(slot >= j, total - total[:, j : j + 1, :], -1e30)
        score = jnp.sum(q3 * k3[:, j : j + 1, :] * jnp.exp(apart), axis=-1, keepdims=True)
        out = out + score * v3[:, j : j + 1, :]
    last = total[:, steps - 1 : steps, :]
    wk_ref[...] = (k3 * jnp.exp(last - total)).reshape(rows, key_dim).astype(BF)
    v_ref[...] = v.astype(BF)
    end_ref[...] = jnp.exp(last)
    side_ref[...] = side
    weighted = (q3 * jnp.exp(total)).reshape(rows, key_dim).astype(BF)
    carried = [
        dot(weighted[s * steps : (s + 1) * steps], state[s].astype(BF)) for s in range(seqs)
    ]
    out = out.reshape(rows, value_dim) + jnp.concatenate(carried, axis=0)
    scale = lax.rsqrt(jnp.mean(out * out, axis=-1, keepdims=True) + EPS)
    silu = r / (1.0 + jnp.exp(-r))
    g_ref[...] = (out * scale * row_of(hs_ref, layer).astype(F32) * silu * live[:, :1]).astype(BF)


def call_recur(meta, full_width, lens, parts, shift, extra, head_scale, state, steps):
    seqs, key_dim, value_dim = state.shape
    rows = seqs * steps
    mine, _, up, down = parts
    first = pl.BlockSpec((1, *mine.shape[1:]), lambda *_: (0, 0, 0, 0))
    out_shape = [
        jax.ShapeDtypeStruct((rows, value_dim), BF),
        jax.ShapeDtypeStruct((rows, key_dim), BF),
        jax.ShapeDtypeStruct((rows, value_dim), BF),
        jax.ShapeDtypeStruct((seqs, 1, key_dim), F32),
        jax.ShapeDtypeStruct((rows, SIDE), F32),
    ]
    return pl.pallas_call(
        functools.partial(recur, full_width, steps),
        grid_spec=pltpu.PrefetchScalarGridSpec(
            num_scalar_prefetch=2,
            grid=(1,),
            in_specs=[
                first,
                first,
                whole(up.shape),
                whole(down.shape),
                whole(shift.shape),
                whole((rows, 1)),
                whole(head_scale.shape),
                whole(state.shape),
            ],
            out_specs=[whole(o.shape) for o in out_shape],
        ),
        out_shape=out_shape,
        compiler_params=params("arbitrary"),
        name="recur",
    )(meta, lens, *parts, shift, extra, head_scale, state)


def plan(steps, side_ref, where_ref):
    side = side_ref[...]
    rows = where_ref.shape[1]
    owners = where_ref.shape[0]
    n = side.shape[0]
    lens_all = jnp.broadcast_to(side[:, 2:3], side.shape).astype(BF)
    seq_of = lax.broadcasted_iota(jnp.int32, (n, owners * rows), 1) // steps
    seq = lax.broadcasted_iota(jnp.int32, (n, owners * rows), 0)
    before = (seq < seq_of).astype(F32).astype(BF)
    same = (seq == seq_of).astype(F32).astype(BF)
    over = (((0,), (0,)), ((), ()))
    start = lax.dot_general(lens_all, before, over, preferred_element_type=F32)[:8]
    length = lax.dot_general(lens_all, same, over, preferred_element_type=F32)[:8]
    t = lax.rem(lax.broadcasted_iota(jnp.int32, start.shape, 1), steps).astype(F32)
    spot = jnp.where(t < length, start + t, -1.0)
    for d in range(owners):
        where_ref[d : d + 1, :] = spot[:1, d * rows : (d + 1) * rows]


def call_plan(steps, owners, side):
    out = jax.ShapeDtypeStruct((owners, side.shape[0]), F32)
    return pl.pallas_call(
        functools.partial(plan, steps),
        grid=(1,),
        in_specs=[whole(side.shape)],
        out_specs=whole(out.shape),
        out_shape=out,
        compiler_params=params("arbitrary"),
        name="plan",
    )(side)


def load(layer, after_ref, state_hbm, out_ref, sem):
    copy = pltpu.make_async_copy(state_hbm.at[layer], out_ref, sem)
    copy.start()
    copy.wait()


def call_load(layer, after, state):
    return pl.pallas_call(
        functools.partial(load, layer),
        grid=(1,),
        in_specs=[whole(after.shape), pl.BlockSpec(memory_space=pltpu.MemorySpace.HBM)],
        out_specs=pl.BlockSpec(memory_space=pltpu.MemorySpace.VMEM),
        out_shape=pltpu.VMEM(state.shape[1:], F32),
        scratch_shapes=[pltpu.SemaphoreType.DMA],
        compiler_params=params("arbitrary"),
        name="load_state",
    )(after, in_hbm(state))


def update(steps, wk_ref, v_ref, end_ref, state_ref, *refs):
    out_ref = refs[-1]
    for s in range(state_ref.shape[0]):
        keys = wk_ref[s * steps : (s + 1) * steps, :]
        values = v_ref[s * steps : (s + 1) * steps, :]
        fresh = lax.dot_general(keys, values, (((0,), (0,)), ((), ())), preferred_element_type=F32)
        end = end_ref[s]
        keep = jnp.transpose(jnp.broadcast_to(end, (end.shape[1], end.shape[1])))[:, :1]
        out_ref[0, s] = keep * state_ref[s] + fresh


def call_update(layer, layers, steps, wk, v, end, state, previous):
    seqs, key_dim, value_dim = state.shape
    step_seqs = 4
    block = pl.BlockSpec((1, step_seqs, key_dim, value_dim), lambda i: (layer, i, 0, 0))
    operands = [wk, v, end, state]
    in_specs = [
        pl.BlockSpec((step_seqs * steps, key_dim), lambda i: (i, 0)),
        pl.BlockSpec((step_seqs * steps, value_dim), lambda i: (i, 0)),
        pl.BlockSpec((step_seqs, 1, key_dim), lambda i: (i, 0, 0)),
        pl.BlockSpec((step_seqs, key_dim, value_dim), lambda i: (i, 0, 0)),
    ]
    alias = {}
    if previous is not None:
        operands.append(previous)
        in_specs.append(pl.BlockSpec(memory_space=pl.ANY))
        alias = {4: 0}
    return pl.pallas_call(
        functools.partial(update, steps),
        grid=(seqs // step_seqs,),
        in_specs=in_specs,
        out_specs=block,
        out_shape=jax.ShapeDtypeStruct((layers, *state.shape), F32),
        input_output_aliases=alias,
        compiler_params=params("arbitrary"),
        name="update_state",
    )(*operands)


def target_ids(meta, shape, span):
    row = lax.broadcasted_iota(jnp.int32, shape, 0)
    block = lax.rem(meta[8] + row // (ROUNDS * span), ROUNDS) + ROUNDS * lax.rem(row // span, ROUNDS)
    return (block * span + lax.rem(row, span)).astype(F32)


def close(tp, meta, where_ref, *refs):
    *g_refs, c_ref, own, plus, minus, far = refs
    rows = where_ref.shape[1]
    n = own.shape[0]
    count = n * ROUNDS
    span = count // tp
    ids = target_ids(meta, (count, rows), span)
    gathered = jnp.zeros((count, c_ref.shape[1]), F32)
    i = 0
    for g in g_refs:
        for b in range(g.shape[0]):
            chosen = (ids == where_ref[pl.ds(meta[i], 1), :]).astype(F32).astype(BF)
            gathered = gathered + dot(chosen, g[b])
            i += 1
    y = dot(gathered.astype(BF), c_ref[0])
    own[...] = y[:n]
    plus[...] = y[n : 2 * n].astype(BF)
    far[...] = y[2 * n : 3 * n].astype(BF)
    minus[...] = y[3 * n :].astype(BF)


def call_close(tp, meta, where, gs, closing, live_rows):
    width = closing.shape[2]
    n = live_rows // ROUNDS
    out_shape = [
        jax.ShapeDtypeStruct((n, width), F32),
        jax.ShapeDtypeStruct((n, width), BF),
        jax.ShapeDtypeStruct((n, width), BF),
        jax.ShapeDtypeStruct((n, width), BF),
    ]
    return pl.pallas_call(
        functools.partial(close, tp),
        grid_spec=pltpu.PrefetchScalarGridSpec(
            num_scalar_prefetch=1,
            grid=(1,),
            in_specs=[
                whole(where.shape),
                *(whole(g.shape) for g in gs),
                pl.BlockSpec((1, *closing.shape[1:]), lambda i, meta: (meta[10], 0, 0)),
            ],
            out_specs=[whole(o.shape) for o in out_shape],
        ),
        out_shape=out_shape,
        compiler_params=params("arbitrary"),
        name="close",
    )(meta, where, *gs, closing)


def own_rows(span, meta, where_ref, x_ref, out_ref):
    rows = where_ref.shape[1]
    ids = target_ids(meta, (out_ref.shape[0], rows), span)
    total = jnp.zeros(out_ref.shape, F32)
    for d in range(where_ref.shape[0]):
        chosen = (ids == where_ref[d : d + 1, :]).astype(F32).astype(BF)
        total = total + dot(chosen, x_ref[d * rows : (d + 1) * rows, :])
    out_ref[...] = total.astype(BF)


def call_own_rows(tp, meta, where, x, live_rows):
    out = jax.ShapeDtypeStruct((live_rows // ROUNDS, x.shape[1]), BF)
    return pl.pallas_call(
        functools.partial(own_rows, live_rows // tp),
        grid_spec=pltpu.PrefetchScalarGridSpec(
            num_scalar_prefetch=1,
            grid=(1,),
            in_specs=[whole(where.shape), whole(x.shape)],
            out_specs=whole(out.shape),
        ),
        out_shape=out,
        compiler_params=params("arbitrary"),
        name="own_rows",
    )(meta, where, x)


def to_chip(x, step):
    n = lax.axis_size("dp")
    return lax.ppermute(x, "dp", [(d, (d + 2 * step) % n) for d in range(n)])


def to_core(x):
    n = lax.axis_size("dp")
    return lax.ppermute(x, "dp", [(d, d ^ 1) for d in range(n)])


def along(x, step):
    n = lax.axis_size("tp")
    return lax.ppermute(x, "tp", [(i, (i + step) % n) for i in range(n)])


def across(x, flip):
    n = lax.axis_size("tp")
    return lax.ppermute(x, "tp", [(i, ROUNDS * ((i // ROUNDS) ^ flip) + i % ROUNDS) for i in range(n)])


def dp_sum(send, mine, fetch):
    core = to_core(send)

    def both(j, h):
        return mine[j, h].astype(F32) + core[j, h].astype(F32)

    far_a = to_chip(both(2, 0).astype(BF), 1)
    far_b = to_chip(both(2, 1).astype(BF), -1)
    up = jnp.stack([both(1, 0) + far_a.astype(F32), both(1, 1)]).astype(BF)
    down = jnp.stack([both(3, 0), both(3, 1) + far_b.astype(F32)]).astype(BF)
    state = fetch(far_b[:8, :128])
    up, down = to_chip(up, 1), to_chip(down, -1)
    up, state = lax.optimization_barrier((up, state))
    return (mine, core, up, down), state


def dp_gather(g):
    far = to_chip(g, -2)
    near = jnp.stack([g, to_chip(g, -1), far, to_chip(g, 1)])
    return near, to_core(near)


def tp_sum(parts, x_own, update):
    own, plus, minus, far = parts
    total = own + along(far, 2).astype(F32)
    total = total + along(plus, 1).astype(F32) + along(minus, -1).astype(F32)
    total = total.astype(BF)
    half = total.shape[1] // 2
    left, right = total[:, :half], total[:, half:]

    def add(a, b):
        return (a.astype(F32) + b.astype(F32)).astype(BF)

    x_own, total, state = update(x_own, total)
    got_left, got_right = across(left, 1), across(right, 3)
    got_left, x_own = lax.optimization_barrier((got_left, x_own))
    left, right = add(left, got_left), add(right, got_right)
    got_left, got_right = across(left, 3), across(right, 1)
    mixed = jnp.concatenate(
        [left.astype(F32) + got_left.astype(F32), right.astype(F32) + got_right.astype(F32)], axis=1
    )
    return (x_own.astype(F32) + mixed).astype(BF), state


def tp_gather(own):
    far = along(own, -2)
    plus = along(own, -1)
    minus = along(own, 1)
    return own, plus, minus, far


def shards(
    skip_path_activations,
    novel_lengths_per_sequence,
    input_normalizer_scales,
    question_projector,
    lookup_projector,
    payload_projector,
    emitted_valve_projector,
    keeping_valve_projector,
    keeping_valve_shift,
    additional_dwindle_exponent,
    headwise_normalizer_scales,
    closing_projector,
    earlier_recurrence_grid,
):
    streams, steps, width = skip_path_activations.shape
    dp, tp = lax.axis_size("dp"), lax.axis_size("tp")
    chips = dp // 2
    full_width = width * dp
    live_rows = streams * steps // 2
    x = skip_path_activations.reshape(streams * steps, width)
    lens = novel_lengths_per_sequence
    gain = input_normalizer_scales
    weights = (
        question_projector,
        lookup_projector,
        payload_projector,
        emitted_valve_projector,
        keeping_valve_projector,
    )
    layers, seqs, heads, key_dim, value_dim = earlier_recurrence_grid.shape
    state = earlier_recurrence_grid.reshape(layers, seqs * heads, key_dim, value_dim)
    extra = additional_dwindle_exponent.reshape(seqs * steps, 1)

    me = lax.axis_index("dp")
    slot = lax.iota(jnp.int32, 32)
    side_core = (slot // chips) % 2
    owner = 2 * ((me // 2 + slot) % chips) + jnp.where(slot < 16, (me % 2) ^ side_core, side_core)
    meta = jnp.where(slot == 8, lax.axis_index("tp"), jnp.where(slot == 9, me, owner)).astype(jnp.int32)
    metas = [jnp.where(slot == 10, layer, meta) for layer in range(layers)]
    other = meta ^ (slot < 2 * chips)

    new_state = None
    where = x_own = pieces = None
    for layer in range(layers):
        if layer == 0:
            run = lambda order: call_project_first(layer, order, in_hbm(lens), x, gain, weights, chips)
        else:
            run = lambda order: call_project_next(layer, order, where, pieces, gain, weights, chips)
        send, mine = [run(order) for order in (other, metas[layer])]
        parts, held = dp_sum(send, mine, lambda after: call_load(layer, after, state))
        g, wk, v, end, side = call_recur(
            metas[layer], full_width, lens, parts, keeping_valve_shift, extra,
            headwise_normalizer_scales, held, steps,
        )
        if layer == 0:
            where = call_plan(steps, dp, side)
            x_own = call_own_rows(tp, meta, where, x, live_rows)
        sums = call_close(tp, metas[layer], where, dp_gather(g), closing_projector, live_rows)

        def update(own, total):
            total, keys = lax.optimization_barrier((total, wk))
            fresh = call_update(layer, layers, steps, keys, v, end, held, new_state)
            own, fresh = lax.optimization_barrier((own, fresh))
            return own, total, fresh

        x_own, new_state = tp_sum(sums, x_own, update)
        pieces = tp_gather(x_own)
    stream = call_finish(meta, where, pieces, x)
    return (
        stream.reshape(streams, steps, width),
        new_state.reshape(earlier_recurrence_grid.shape),
    )


def solution(mesh):
    in_specs = (
        P("grp", None, "dp"),
        P(("grp", "dp")),
        P(None, "dp"),
        P(None, "dp", "tp"),
        P(None, "dp", "tp"),
        P(None, "dp", "tp"),
        P(None, "dp", "tp"),
        P(None, "dp", "tp"),
        P(None, "tp"),
        P(("grp", "dp"), None, "tp"),
        P(),
        P(None, "tp", "dp"),
        P(None, ("grp", "dp"), "tp", None, None),
    )
    out_specs = (P("grp", None, "dp"), P(None, ("grp", "dp"), "tp", None, None))
    return jax.shard_map(shards, mesh=mesh, in_specs=in_specs, out_specs=out_specs, check_vma=False)
```
